512 devices in a mesh: sp: 32 (over z, x), tp: 16 (over y, core).
Axes of the slice: x: 4, y: 8, z: 8, core: 2. Of those that a mesh axis runs over, the one named last changes fastest.
Arguments:
- stream_in: bfloat16 [4096, 2048], P('sp'), may hold values from -8 to 8
- out_cot: bfloat16 [4096, 2048], P('sp'), may hold values from -6 to 6
- route_experts: int32 [4096, 2], P('sp'), may hold values from 0 to 31, all different within a row; in each aligned block of 128 rows (0 to 127, 128 to 255, ...) at most 16 rows name the same one
- route_weights: float32 [4096, 2], P('sp'), may hold values from 0.1 to 1
- w_gate: bfloat16 [32, 2048, 2048], P('sp', None, 'tp'), may hold values from -0.125 to 0.125
- w_up: bfloat16 [32, 2048, 2048], P('sp', None, 'tp'), may hold values from -0.125 to 0.125
- w_down: bfloat16 [32, 2048, 2048], P('sp', 'tp'), may hold values from -0.125 to 0.125
- w_proj: bfloat16 [2048, 1024], P(None, 'tp'), may hold values from -0.1875 to 0.1875
- conv_value: bfloat16 [1024, 4096], P('tp', 'sp'), may hold values from -6 to 6
- conv_gate: bfloat16 [1024, 4096], P('tp', 'sp'), may hold values from -8 to 8
- conv_taps: float32 [31, 1024], P(None, 'tp'), may hold values from -1 to 1
- conv_result: bfloat16 [1024, 4096], P('tp', 'sp'), may hold values from -100 to 100
- channel_norm_gain: float32 [1024], P('tp'), may hold values from 0.1 to 1.9
Outputs:
- grad_gate: bfloat16 [32, 2048, 2048], P('sp', None, 'tp')
- grad_up: bfloat16 [32, 2048, 2048], P('sp', None, 'tp')
- grad_down: bfloat16 [32, 2048, 2048], P('sp', 'tp')
- grad_stream: bfloat16 [4096, 2048], P('sp')
- grad_proj: float32 [2048, 1024], P('sp', 'tp')
- grad_value: bfloat16 [1024, 4096], P('tp', 'sp')
- grad_gate_in: bfloat16 [1024, 4096], P('tp', 'sp')
The draws below stay inside these ranges and needn't reach their ends.
Inputs may be any that keep to these rules, and one draw needn't show every extreme that they name: `route_experts`: each row names 2 different experts; within each aligned block of 128 rows no expert is named by more than 16 rows, and at least one block reaches that bound for some expert.
All inputs are finite; a program needn't handle non-finite values.
Results may differ from the reference program's by a relative error of at most 0.025.
Values may be sent and summed in bfloat16 or wider, within the bound.
No kernel may reach another device: no remote copies, remote signals or barrier semaphores. Data moves between devices by JAX's collectives and lax.ppermute only.
A program may use at most 64 MiB of HBM per device.

```python
import math
import jax
import jax.numpy as jnp
import numpy as np
from jax import lax

D = 2048
FF = 2048
CONV_CHANNELS = 1024
CONV_W = 31
TOP = 2
T_DEV = 128
EXPERTS = 32
TOKENS = 4096
CAP = 16
N_SP = 32
N_TP = 16


def draw_conv_result(key, part):
    first_key, second_key, third_key = jax.random.split(jax.random.fold_in(key, 17), 3)
    base = jnp.clip(jax.random.normal(first_key, (CONV_CHANNELS, TOKENS), jnp.float32), -6.0, 6.0)
    channel_pos = jnp.arange(CONV_CHANNELS, dtype=jnp.float32) / CONV_CHANNELS
    rough = jax.random.uniform(second_key, (CONV_CHANNELS, 1), jnp.float32, 0.5, 1.5)
    shift_noise = jnp.clip(jax.random.normal(third_key, (1, TOKENS), jnp.float32), -4.0, 4.0)
    scales = jnp.exp(jnp.log(3.0) * channel_pos)[:, None] * rough
    offset = shift_noise
    return (base * scales + offset).astype(jnp.bfloat16)


def spiked(values, rng, source, target, shards_of, factor):
    def block_of(dim):
        return (jnp.arange(values.shape[dim]) // (values.shape[dim] // shards_of)).reshape((-1,) + (1,) * (values.ndim - 1 - dim))

    near = jax.random.permutation(rng, shards_of)[block_of(target)]
    second = (block_of(target) + shards_of // 2) % shards_of
    return jnp.where((block_of(source) == near) | (block_of(source) == second), factor * values, values)


def steps_of(key, extent, cuts, smallest, top_value):
    def one(dim, parts):
        heights = jax.random.uniform(jax.random.fold_in(jax.random.fold_in(key, 6), dim), (parts,), jnp.float32, smallest / len(cuts), top_value / len(cuts))
        return jnp.repeat(jnp.exp(heights), extent[dim] // parts).reshape((-1,) + (1,) * (len(extent) - dim - 1))

    gain = one(*cuts[0])
    for cut in cuts[1:]:
        gain = gain * one(*cut)
    return gain


def deal_out(own_key, own, number, rows, count, top, reach, skew):
    ranking = jax.random.permutation(own_key, count)
    heavy_load, ordinary = load_shares(count, rows * top, reach, skew, True), load_shares(count, rows * top, reach, skew, False)
    places = jnp.arange(count)

    def named(sizes, turn):
        used = int((sizes > 0).sum())
        fixed = max(1, used // 4)
        moved = fixed + (places - fixed + turn * (used - fixed)) % max(1, count - fixed)
        return jnp.zeros((count,), jnp.int32).at[ranking[jnp.where(places < fixed, places, moved)]].set(jnp.asarray(sizes, jnp.int32))

    sizes = jnp.where(number % 4 == 0, named(heavy_load, number // 4), named(ordinary, number - number // 4 - 1))
    mixed = jax.random.permutation(jax.random.fold_in(own, 3), count)
    donor, sink = mixed[0:count // 2 * 2:2], mixed[1:count // 2 * 2:2]
    slack = jnp.minimum(sizes[donor] - 1, reach - sizes[sink]) // 2
    slack = jnp.where((donor == ranking[0]) | (sink == ranking[0]) | (sizes[sink] == 0), 0, jnp.maximum(slack, 0))
    moved = jax.random.randint(jax.random.fold_in(own, 4), (count // 2,), 0, 1 << 20) % (slack + 1)
    sizes = sizes.at[donor].add(-moved).at[sink].add(moved)
    labels = jnp.searchsorted(jnp.cumsum(sizes), jnp.arange(rows * top), side="right").astype(jnp.int32)
    listing = labels.reshape(top, rows).T
    listing = listing[jax.random.permutation(jax.random.fold_in(own, 1), rows)]
    turn = jax.random.randint(jax.random.fold_in(own, 2), (rows, 1), 0, top)
    return jnp.take_along_axis(listing, (jnp.arange(top)[None, :] + turn) % top, axis=1)


def load_shares(amount, total, most, lean, full):
    portions = [(1 << 20) // math.isqrt(grade ** lean) + 1 for grade in range(1, amount + 1)]
    largest = most if full else min(most, max(-(-total // amount), total * portions[0] // sum(portions)))
    least = 1 if total - largest >= amount - 1 else 0
    given, spare = [largest] + [least] * (amount - 1), total - largest - least * (amount - 1)
    while spare > 0:
        candidates = [i for i in range(1, amount) if given[i] < largest] or [i for i in range(1, amount) if given[i] < most]
        mass, budget = sum([portions[i] for i in candidates]), spare
        for i in candidates:
            more = min(most - given[i], max(1, budget * portions[i] // mass), spare)
            given[i] = given[i] + more
            spare = spare - more
    return np.array(given)


def centred(key, extent, width, most, cuts=(), kind=jnp.bfloat16):
    entries = jax.random.normal(key, extent, jnp.float32) * width
    if len(cuts) > 0:
        entries = steps_of(key, extent, cuts, -0.22, 0.18) * entries
    return jnp.clip(entries, min=-most, max=most).astype(kind)


def gaussian_with(rng, shape, deviation, most, cuts, heavy, kind=jnp.bfloat16):
    values = deviation * jax.random.normal(rng, shape, jnp.float32)
    if cuts:
        values = values * steps_of(rng, shape, cuts, -0.22, 0.18)
    return jnp.clip(spiked(values, jax.random.fold_in(rng, 3), *heavy), -most, most).astype(kind)


def setup_inputs(seed: int = 0) -> dict:
    key_list = jax.random.split(jax.random.key(seed), 14)
    stream_in = centred(key_list[0], (TOKENS, D), 1.25, 8.0, ((0, 32),))
    out_cot = gaussian_with(key_list[1], (TOKENS, D), 1.0, 6.0, ((0, 32),), (0, 1, 32, 2.75))
    route_experts_keys = jax.random.split(jax.random.fold_in(key_list[2], 1), TOKENS // T_DEV)
    route_experts_turns = jax.random.permutation(jax.random.fold_in(key_list[2], 3), TOKENS // T_DEV)
    route_experts = jax.vmap(lambda own, number: deal_out(jax.random.fold_in(key_list[2], 2), own, number, T_DEV, EXPERTS, TOP, CAP, 2))(route_experts_keys, route_experts_turns).reshape((TOKENS, TOP))
    route_weights = jnp.clip(0.1 + 0.9 * jax.random.uniform(key_list[3], (TOKENS, TOP), jnp.float32) ** steps_of(key_list[3], (TOKENS, TOP), ((0, 32),), -0.2, 0.2), 0.1, 1.0)
    w_gate = centred(key_list[4], (EXPERTS, D, FF), D ** -0.5, 0.125, ((0, 32), (2, 16)))
    w_up = centred(key_list[5], (EXPERTS, D, FF), D ** -0.5, 0.125, ((0, 32), (2, 16)))
    w_down = centred(key_list[6], (EXPERTS, FF, D), FF ** -0.5, 0.125, ((0, 32), (1, 16)))
    w_proj = centred(key_list[7], (D, CONV_CHANNELS), CONV_CHANNELS ** -0.5, 0.1875, ((1, 16),))
    conv_value = centred(key_list[8], (CONV_CHANNELS, TOKENS), 1.0, 6.0, ((0, 16), (1, 32)))
    conv_gate = centred(key_list[9], (CONV_CHANNELS, TOKENS), 1.5, 8.0, ((0, 16), (1, 32)))
    conv_taps = centred(key_list[10], (CONV_W, CONV_CHANNELS), CONV_W ** -0.5, 1.0, ((1, 16),), jnp.float32)
    conv_result = draw_conv_result(jax.random.fold_in(key_list[13], 71), 0)
    channel_norm_gain = jnp.clip(1.0 + 0.18 * jax.random.normal(key_list[12], (CONV_CHANNELS,), jnp.float32), 0.1, 1.9)
    return dict(stream_in=stream_in, out_cot=out_cot, route_experts=route_experts, route_weights=route_weights, w_gate=w_gate, w_up=w_up, w_down=w_down, w_proj=w_proj, conv_value=conv_value, conv_gate=conv_gate, conv_taps=conv_taps, conv_result=conv_result, channel_norm_gain=channel_norm_gain)


norm_eps = 1e-05
clamp_limit = 7.0
alpha_gate = 1.702

def slot_tables(block_routes, experts_all, capacity):
    flat_routes = block_routes.reshape(-1).astype(jnp.int32)
    assigns = flat_routes.shape[0]
    onehot = (flat_routes[:, None] == jnp.arange(experts_all, dtype=jnp.int32)[None, :]).astype(jnp.int32)
    before = jnp.cumsum(onehot, axis=0) - onehot
    rank_in = lax.optimization_barrier(jnp.sum(before * onehot, axis=1)).astype(jnp.int32)
    slot_of = (flat_routes * capacity + rank_in).astype(jnp.int32)
    source_of = jnp.full((experts_all * capacity,), -1, jnp.int32).at[slot_of].set(jnp.arange(assigns, dtype=jnp.int32))
    return (slot_of, source_of)

def one_expert(operands):
    rows_in, cot_in, gate_mat, up_mat, down_mat = operands
    pre_gate = jnp.dot(rows_in, gate_mat, preferred_element_type=jnp.float32)
    pre_up = jnp.dot(rows_in, up_mat, preferred_element_type=jnp.float32)
    glu_part = jnp.minimum(pre_gate, clamp_limit)
    lin_part = jnp.clip(pre_up, -clamp_limit, clamp_limit)
    sig_glu = jax.nn.sigmoid(alpha_gate * glu_part)
    activated = (glu_part * sig_glu * (lin_part + 1.0)).astype(jnp.bfloat16)
    grad_act = lax.dot_general(cot_in, down_mat, (((1,), (1,)), ((), ())), preferred_element_type=jnp.float32)
    slope = sig_glu + alpha_gate * glu_part * sig_glu * (1.0 - sig_glu)
    grad_pre_gate = jnp.where(pre_gate < clamp_limit, grad_act * (lin_part + 1.0) * slope, 0.0).astype(jnp.bfloat16)
    grad_pre_up = jnp.where(jnp.abs(pre_up) < clamp_limit, grad_act * glu_part * sig_glu, 0.0).astype(jnp.bfloat16)
    dims = (((0,), (0,)), ((), ()))
    grad_down = lax.dot_general(activated, cot_in, dims, preferred_element_type=jnp.float32).astype(jnp.bfloat16)
    grad_gate = lax.dot_general(rows_in, grad_pre_gate, dims, preferred_element_type=jnp.float32).astype(jnp.bfloat16)
    grad_up = lax.dot_general(rows_in, grad_pre_up, dims, preferred_element_type=jnp.float32).astype(jnp.bfloat16)
    row_count = rows_in.shape[0]
    group_width = FF // N_TP
    partial_sum = jnp.einsum('rpf,dpf->prd', grad_pre_gate.reshape(row_count, N_TP, group_width).astype(jnp.float32), gate_mat.reshape(D, N_TP, group_width).astype(jnp.float32))
    partial_sum = partial_sum + jnp.einsum('rpf,dpf->prd', grad_pre_up.reshape(row_count, N_TP, group_width).astype(jnp.float32), up_mat.reshape(D, N_TP, group_width).astype(jnp.float32))
    rounded = lax.optimization_barrier(partial_sum.astype(jnp.bfloat16))
    route_grad = lax.optimization_barrier(jnp.sum(rounded.astype(jnp.float32), axis=0)).astype(jnp.bfloat16)
    return (grad_gate, grad_up, grad_down, route_grad)

def reference(stream_in, out_cot, route_experts, route_weights, w_gate, w_up, w_down, w_proj, conv_value, conv_gate, conv_taps, conv_result, channel_norm_gain):
    block_routes = route_experts.reshape(N_SP, T_DEV, TOP)
    slot_of, source_of = jax.vmap(lambda routes_one: slot_tables(routes_one, EXPERTS, CAP))(block_routes)
    occupied = source_of >= 0
    source_safe = jnp.maximum(source_of, 0)
    offsets = (jnp.arange(N_SP, dtype=jnp.int32) * T_DEV)[:, None]
    token_of = (source_safe // TOP + offsets).astype(jnp.int32)
    weight_flat = route_weights.reshape(N_SP, T_DEV * TOP)
    slot_weight = jnp.where(occupied, jnp.take_along_axis(weight_flat, source_safe, axis=1), 0.0)
    row_buffer = jnp.where(occupied[..., None], stream_in[token_of], jnp.zeros((), jnp.bfloat16)).astype(jnp.bfloat16)
    cot_buffer = (slot_weight[..., None] * out_cot[token_of].astype(jnp.float32)).astype(jnp.bfloat16)
    row_buffer = row_buffer.reshape(N_SP, EXPERTS, CAP, D).transpose(1, 0, 2, 3).reshape(EXPERTS, N_SP * CAP, D)
    cot_buffer = cot_buffer.reshape(N_SP, EXPERTS, CAP, D).transpose(1, 0, 2, 3).reshape(EXPERTS, N_SP * CAP, D)
    grad_gate, grad_up, grad_down, route_grad = lax.map(one_expert, (row_buffer, cot_buffer, w_gate, w_up, w_down))
    returned = route_grad.reshape(EXPERTS, N_SP, CAP, D).transpose(1, 0, 2, 3).reshape(N_SP, EXPERTS * CAP, D)
    per_route = jnp.take_along_axis(returned, slot_of[..., None], axis=1).astype(jnp.float32)
    per_route = per_route.reshape(TOKENS, TOP, D)
    grad_stream = (out_cot.astype(jnp.float32) + lax.optimization_barrier(jnp.sum(per_route, axis=1))).astype(jnp.bfloat16)
    conv_float = conv_result.astype(jnp.float32)
    chan_mean = lax.optimization_barrier(jnp.sum(conv_float, axis=0)) / CONV_CHANNELS
    chan_var = lax.optimization_barrier(jnp.sum(conv_float * conv_float, axis=0)) / CONV_CHANNELS - chan_mean * chan_mean
    inverse_deviation = lax.rsqrt(chan_var + norm_eps)
    mean_removed = (conv_float - chan_mean) * inverse_deviation
    normalized_rows = mean_removed * channel_norm_gain[:, None]
    sigmoid_of_norm = jax.nn.sigmoid(normalized_rows)
    hidden = (normalized_rows * sigmoid_of_norm).astype(jnp.bfloat16)
    grad_proj = lax.dot_general(grad_stream, hidden, (((0,), (1,)), ((), ())), preferred_element_type=jnp.float32)
    hidden_gradient = lax.dot_general(w_proj, grad_stream, (((0,), (1,)), ((), ())), preferred_element_type=jnp.float32)
    normed_input_gradient = hidden_gradient * sigmoid_of_norm * (1.0 + normalized_rows * (1.0 - sigmoid_of_norm)) * channel_norm_gain[:, None]
    average_products = lax.optimization_barrier(jnp.sum(normed_input_gradient, axis=0)) / CONV_CHANNELS
    cross_products = lax.optimization_barrier(jnp.sum(normed_input_gradient * mean_removed, axis=0)) / CONV_CHANNELS
    conv_output_gradient = inverse_deviation * (normed_input_gradient - average_products - mean_removed * cross_products)
    extended = jnp.concatenate([conv_output_gradient, jnp.zeros((CONV_CHANNELS, CONV_W - 1), jnp.float32)], axis=1)
    grad_gated = jnp.zeros((CONV_CHANNELS, TOKENS), jnp.float32)
    for tap_index in range(CONV_W):
        grad_gated = grad_gated + conv_taps[tap_index][:, None] * extended[:, tap_index:tap_index + TOKENS]
    gate_sig = jax.nn.sigmoid(conv_gate.astype(jnp.float32))
    grad_value = (grad_gated * gate_sig).astype(jnp.bfloat16)
    grad_gate_in = (grad_gated * conv_value.astype(jnp.float32) * gate_sig * (1.0 - gate_sig)).astype(jnp.bfloat16)
    return (grad_gate, grad_up, grad_down, grad_stream, grad_proj, grad_value, grad_gate_in)
```

```python
import jax
import jax.numpy as jnp
from jax import lax
from jax.sharding import PartitionSpec as P

norm_eps = 1e-05
clamp_limit = 7.0
alpha_gate = 1.702
bf16 = jnp.bfloat16
f32 = jnp.float32


def dot(a, b, dims):
    return lax.dot_general(a, b, (dims, ((), ())), preferred_element_type=f32)


def swap_cores(value, tp_count):
    return lax.ppermute(value, "tp", [(k, k ^ 1) for k in range(tp_count)])


def swap_chips(value, tp_count):
    return lax.ppermute(value, "tp", [(k, k ^ 2) for k in range(tp_count)])


def packed_total(arrays, axis):
    ends = [0]
    for a in arrays:
        ends.append(ends[-1] + a.size)
    flat = jnp.concatenate([a.ravel() for a in arrays])
    copies = jnp.broadcast_to(flat, (lax.axis_size(axis), *flat.shape))
    total = lax.all_to_all(copies, axis, 0, 0, tiled=True).sum(axis=0)
    return tuple((total[b:e].reshape(a.shape) for a, b, e in zip(arrays, ends, ends[1:])))


def slot_choice(routes, weights, experts, capacity, share, part):
    count, top = routes.shape
    by_rank = routes.T
    before = jnp.triu(jnp.ones((count, count), bf16), 1)
    base = jnp.zeros((experts, 1), f32)
    slots = lax.broadcasted_iota(jnp.int32, (experts * share, count), 0)
    chosen = []
    for k in range(top):
        hot = by_rank[k][None, :] == lax.broadcasted_iota(jnp.int32, (experts, count), 0)
        ahead = dot(hot.astype(bf16), before, ((1,), (0,))) + base
        base = base + jnp.sum(hot.astype(f32), axis=1, keepdims=True)
        rank = jnp.sum(jnp.where(hot, ahead, 0.0), axis=0).astype(jnp.int32) - part * share
        held = (rank >= 0) & (rank < share)
        slot = jnp.where(held, by_rank[k] * share + rank, -1)
        chosen.append(slots == slot[None, :])
    weight = sum(jnp.where(c, weights.T[k][None, :], 0.0) for k, c in enumerate(chosen))
    picked = chosen[0]
    for c in chosen[1:]:
        picked = picked | c
    return picked.astype(bf16), jnp.sum(weight, axis=1, keepdims=True)


def body(
    stream_in,
    out_cot,
    route_experts,
    route_weights,
    w_gate,
    w_up,
    w_down,
    w_proj,
    conv_value,
    conv_gate,
    conv_taps,
    conv_result,
    channel_norm_gain,
):
    sp_count = lax.axis_size("sp")
    tp_count = lax.axis_size("tp")
    chips = tp_count // 2
    tp = lax.axis_index("tp")
    core = tp % 2
    part = (tp // 2) % 2
    experts = w_gate.shape[0] * sp_count
    tokens, width = stream_in.shape
    top = route_experts.shape[1]
    capacity = 2 * top * tokens // experts
    share = capacity // 2
    rows = sp_count * share
    half = width // 2
    cols = width // tp_count
    hid = w_gate.shape[2]

    def halves(x, axis):
        shape = x.shape[:axis] + (chips, 2, cols) + x.shape[axis + 1 :]
        x = x.reshape(shape)
        mine = lax.dynamic_index_in_dim(x, core, axis + 1, keepdims=False)
        other = lax.dynamic_index_in_dim(x, 1 - core, axis + 1, keepdims=False)
        flat = shape[:axis] + (half,) + shape[axis + 3 :]
        return mine.reshape(flat), other.reshape(flat)

    w_own = jnp.stack([w_gate[0], w_up[0], w_down[0].T])
    w_own = jnp.concatenate(halves(w_own, 1), axis=1)
    w_far = swap_chips(w_own, tp_count)

    picked, slot_weight = slot_choice(
        route_experts, route_weights, experts, capacity, share, part
    )
    row_half = halves(stream_in, 1)[0]
    cot_half = halves(out_cot, 1)[0]
    row_out = dot(picked, row_half, ((1,), (0,))).astype(bf16)
    cot_out = (slot_weight * dot(picked, cot_half, ((1,), (0,)))).astype(bf16)
    sent = jnp.concatenate(
        [row_out.reshape(experts, share, half), cot_out.reshape(experts, share, half)], axis=1
    )
    mine = lax.all_to_all(sent, "sp", 0, 0, tiled=True)
    other = swap_cores(mine, tp_count)
    both = jnp.concatenate([mine, other], axis=2)
    rows_in = both[:, :share].reshape(rows, width)
    cot_in = both[:, share:].reshape(rows, width)

    w_all = jnp.concatenate([w_own, w_far], axis=2)
    pre_gate = dot(rows_in, w_all[0], ((1,), (0,)))
    pre_up = dot(rows_in, w_all[1], ((1,), (0,)))
    grad_act = dot(cot_in, w_all[2], ((1,), (0,)))
    glu = jnp.minimum(pre_gate, clamp_limit)
    lin = jnp.clip(pre_up, -clamp_limit, clamp_limit)
    sig = jax.nn.sigmoid(alpha_gate * glu)
    activated = (glu * sig * (lin + 1.0)).astype(bf16)
    slope = sig + alpha_gate * glu * sig * (1.0 - sig)
    gate_in = jnp.where(pre_gate < clamp_limit, grad_act * (lin + 1.0) * slope, 0.0).astype(bf16)
    up_in = jnp.where(jnp.abs(pre_up) < clamp_limit, grad_act * glu * sig, 0.0).astype(bf16)

    back = dot(gate_in, w_all[0], ((1,), (1,))) + dot(up_in, w_all[1], ((1,), (1,)))
    from_core = swap_cores(back[:, half:].astype(bf16), tp_count)
    back = (back[:, :half] + from_core.astype(f32)).astype(bf16)

    gate_far = dot(rows_in, gate_in[:, hid:], ((0,), (0,)))
    up_far = dot(rows_in, up_in[:, hid:], ((0,), (0,)))
    down_far = dot(activated[:, hid:], cot_in, ((0,), (0,)))
    far_in = swap_chips(jnp.stack([gate_far, up_far]).astype(bf16), tp_count)
    far_down = swap_chips(down_far.astype(bf16), tp_count)
    gate_own = dot(rows_in, gate_in[:, :hid], ((0,), (0,))) + far_in[0].astype(f32)
    up_own = dot(rows_in, up_in[:, :hid], ((0,), (0,))) + far_in[1].astype(f32)
    down_own = dot(activated[:, :hid], cot_in, ((0,), (0,))) + far_down.astype(f32)

    def in_order(x, axis):
        shape = x.shape[:axis] + (2, chips, cols) + x.shape[axis + 1 :]
        x = x.astype(bf16).reshape(shape)
        x = jnp.where(core == 0, x, jnp.flip(x, axis))
        x = jnp.moveaxis(x, axis, axis + 1)
        return x.reshape(shape[:axis] + (width,) + shape[axis + 3 :])

    grad_gate = in_order(gate_own, 0)[None]
    grad_up = in_order(up_own, 0)[None]
    grad_down = in_order(down_own, 1)[None]

    returned = lax.all_to_all(back.reshape(sp_count, share, half), "sp", 0, 0, tiled=True)
    merged = dot(picked, returned.reshape(experts * share, half), ((0,), (0,)))
    merged = merged.astype(bf16).reshape(tokens, chips, cols).transpose(1, 0, 2)
    same_core = [[2 * k + c for k in range(chips)] for c in range(2)]
    merged = lax.all_to_all(merged, "tp", 0, 0, axis_index_groups=same_core, tiled=True)
    cot_cols = lax.dynamic_slice_in_dim(out_cot, tp * cols, cols, 1)
    stream_part = (cot_cols.astype(f32) + jnp.sum(merged.astype(f32), axis=0)).astype(bf16)
    grad_stream = lax.all_gather(stream_part, "tp", axis=1, tiled=True)

    channels = conv_result.shape[0]
    channel_total = channels * tp_count
    positions = conv_result.shape[1]
    conv_float = conv_result.astype(f32)
    chan_sum, chan_sq = packed_total(
        (jnp.sum(conv_float, axis=0), jnp.sum(conv_float * conv_float, axis=0)), "tp"
    )
    chan_mean = chan_sum / channel_total
    chan_var = chan_sq / channel_total - chan_mean * chan_mean
    inverse_deviation = lax.rsqrt(chan_var + norm_eps)
    centred = (conv_float - chan_mean) * inverse_deviation
    normed = centred * channel_norm_gain[:, None]
    sig_norm = jax.nn.sigmoid(normed)
    hidden = (normed * sig_norm).astype(bf16)

    grad_hidden = dot(w_proj, grad_stream, ((0,), (1,)))
    grad_xhat = (
        grad_hidden * sig_norm * (1.0 + normed * (1.0 - sig_norm)) * channel_norm_gain[:, None]
    )
    mean_one, mean_two = packed_total(
        (jnp.sum(grad_xhat, axis=0), jnp.sum(grad_xhat * centred, axis=0)), "tp"
    )
    grad_conv = inverse_deviation * (
        grad_xhat - mean_one / channel_total - centred * (mean_two / channel_total)
    )

    twice = jnp.concatenate([hidden, hidden], axis=0)
    proj = dot(grad_stream, twice, ((0,), (1,)))
    per = width // sp_count
    proj = proj.reshape(sp_count, 2, per // 2, 2 * channels)
    lane = lax.broadcasted_iota(jnp.int32, (1, 1, 2 * channels), 2)
    packed = jnp.where(lane < channels, proj[:, 0], proj[:, 1]).astype(bf16)
    packed = lax.all_to_all(packed, "sp", 0, 0, tiled=True)
    total = jnp.sum(packed.astype(f32), axis=0)
    grad_proj = jnp.concatenate([total[:, :channels], total[:, channels:]], axis=0)

    taps = conv_taps.shape[0]
    rim = lax.ppermute(
        grad_conv[:, : taps - 1], "sp", [(k, k - 1) for k in range(1, sp_count)]
    )
    extended = jnp.concatenate([grad_conv, rim], axis=1)
    grad_gated = jnp.zeros_like(grad_conv)
    for tap in range(taps):
        grad_gated = grad_gated + conv_taps[tap][:, None] * extended[:, tap : tap + positions]
    gate_sig = jax.nn.sigmoid(conv_gate.astype(f32))
    grad_value = (grad_gated * gate_sig).astype(bf16)
    grad_gate_in = (grad_gated * conv_value.astype(f32) * gate_sig * (1.0 - gate_sig)).astype(bf16)
    return (grad_gate, grad_up, grad_down, grad_stream, grad_proj, grad_value, grad_gate_in)


def solution(mesh):
    return jax.shard_map(
        body,
        mesh=mesh,
        in_specs=(
            P("sp", None),
            P("sp", None),
            P("sp", None),
            P("sp", None),
            P("sp", None, "tp"),
            P("sp", None, "tp"),
            P("sp", "tp", None),
            P(None, "tp"),
            P("tp", "sp"),
            P("tp", "sp"),
            P(None, "tp"),
            P("tp", "sp"),
            P("tp"),
        ),
        out_specs=(
            P("sp", None, "tp"),
            P("sp", None, "tp"),
            P("sp", "tp", None),
            P("sp", None),
            P("sp", "tp"),
            P("tp", "sp"),
            P("tp", "sp"),
        ),
        check_vma=False,
    )
```

```python
import functools

import jax
import jax.numpy as jnp
from jax import lax
from jax.experimental import pallas as pl
from jax.experimental.pallas import tpu as pltpu
from jax.sharding import Mesh
from jax.sharding import PartitionSpec as P

norm_eps = 1e-05
clamp_limit = 7.0
alpha_gate = 1.702
bf16 = jnp.bfloat16
f32 = jnp.float32
LANES = 128


TP = ("chip", "core")
VMEM = pl.BlockSpec(memory_space=pltpu.VMEM)
SMEM = pl.BlockSpec(memory_space=pltpu.SMEM)


def dot(a, b, dims):
    return lax.dot_general(a, b, (dims, ((), ())), preferred_element_type=f32)


NN = ((1,), (0,))
NT = ((1,), (1,))
TN = ((0,), (0,))


def local_kernel(body, outs, *args, specs=None, flops=10**9):
    size = sum(a.size * a.dtype.itemsize for a in args)
    return pl.pallas_call(
        body,
        out_shape=outs,
        in_specs=[VMEM] * len(args) if specs is None else specs,
        out_specs=jax.tree.map(lambda _: VMEM, outs),
        cost_estimate=pl.CostEstimate(flops=flops, bytes_accessed=size, transcendentals=0),
        compiler_params=pltpu.CompilerParams(vmem_limit_bytes=40 * 2**20),
    )(*args)


def shaped(shape, dtype):
    return jax.ShapeDtypeStruct(shape, dtype)


def swap_cores(value):
    return lax.ppermute(value, "core", [(0, 1), (1, 0)])


def swap_chips(value):
    count = lax.axis_size("chip")
    return lax.ppermute(value, "chip", [(k, k ^ 1) for k in range(count)])


def prepare(experts, capacity, share, chips, ids, routes, weights, stream, cot, out, slots):
    top, count = routes.shape
    core, part = ids[0], ids[1]
    before = (
        lax.broadcasted_iota(jnp.int32, (count, count), 0)
        < lax.broadcasted_iota(jnp.int32, (count, count), 1)
    ).astype(bf16)
    named = lax.broadcasted_iota(jnp.int32, (experts, count), 0)
    row = lax.broadcasted_iota(jnp.int32, (experts * share, count), 0)
    base = jnp.zeros((experts, 1), f32)
    picked = jnp.zeros((experts * share, count), jnp.bool_)
    weight = jnp.zeros((experts * share, count), f32)
    for k in range(top):
        route = routes[k : k + 1, :]
        hot = named == route
        ones = jnp.where(hot, 1.0, 0.0)
        ahead = dot(ones.astype(bf16), before, NN) + base
        base = base + jnp.sum(ones, axis=1, keepdims=True)
        rank = jnp.sum(jnp.where(hot, ahead, 0.0), axis=0, keepdims=True).astype(jnp.int32)
        slots[k : k + 1, :] = route * capacity + rank
        local = rank - part * share
        held = (local >= 0) & (local < share)
        mine = row == jnp.where(held, route * share + local, -1)
        picked = picked | mine
        weight = weight + jnp.where(mine, weights[k : k + 1, :], 0.0)
    choice = jnp.where(picked, 1.0, 0.0).astype(bf16)
    scale = jnp.sum(weight, axis=1, keepdims=True)
    half = chips * LANES
    for i in range(chips):
        at = pl.ds(pl.multiple_of((2 * i + core) * LANES, LANES), LANES)
        out[:, i * LANES : (i + 1) * LANES] = dot(choice, stream[:, at], NN).astype(bf16)
        got = dot(choice, cot[:, at], NN)
        out[:, half + i * LANES : half + (i + 1) * LANES] = (scale * got).astype(bf16)


def experts_step(mine, other, own, far, act, gate_in, up_in, back_mine, back_other):
    half = mine.shape[1] // 2
    hid = own.shape[2]
    for h, w in enumerate((own, far)):
        def product(n, at):
            return dot(mine[:, at : at + half], w[n, :half], NN) + dot(
                other[:, at : at + half], w[n, half:], NN
            )

        pre_gate, pre_up, grad_act = product(0, 0), product(1, 0), product(2, half)
        glu = jnp.minimum(pre_gate, clamp_limit)
        lin = jnp.clip(pre_up, -clamp_limit, clamp_limit)
        sig = jax.nn.sigmoid(alpha_gate * glu)
        slope = sig + alpha_gate * glu * sig * (1.0 - sig)
        cols = slice(h * hid, (h + 1) * hid)
        act[:, cols] = (glu * sig * (lin + 1.0)).astype(bf16)
        gate_in[:, cols] = jnp.where(
            pre_gate < clamp_limit, grad_act * (lin + 1.0) * slope, 0.0
        ).astype(bf16)
        up_in[:, cols] = jnp.where(
            jnp.abs(pre_up) < clamp_limit, grad_act * glu * sig, 0.0
        ).astype(bf16)

    def back(at):
        total = 0.0
        for h, w in enumerate((own, far)):
            cols = slice(h * hid, (h + 1) * hid)
            total = total + dot(gate_in[:, cols], w[0, at : at + half], NT)
            total = total + dot(up_in[:, cols], w[1, at : at + half], NT)
        return total

    back_other[...] = back(half).astype(bf16)
    back_mine[...] = back(0)


def finish(capacity, share, chips, data, slots, cot, lean_one, lean_two, out):
    rows, count = data.shape[0], slots.shape[1]
    row = lax.broadcasted_iota(jnp.int32, (rows, count), 0)
    expert = row // (chips * share)
    chip = (row // share) % chips
    key = expert * capacity + (chip % 2) * share + row % share
    hit = (key == slots[0:1, :]) | (key == slots[1:2, :])
    total = dot(jnp.where(hit, 1.0, 0.0).astype(bf16), data[...], TN)
    stream = (cot[...].astype(f32) + total).astype(bf16)
    out[0:count, :] = stream
    wide = stream.astype(f32)
    one = jnp.sum((wide * lean_one[...]).T, axis=0, keepdims=True)
    two = jnp.sum((wide * lean_two[...]).T, axis=0, keepdims=True)
    at = lax.broadcasted_iota(jnp.int32, (16, count), 0)
    both = jnp.where((at // 2) % 2 == 0, one, two)
    high = both.astype(bf16)
    low = (both - high.astype(f32)).astype(bf16)
    out[count : count + 16, :] = jnp.where(at % 2 == 0, high.astype(f32), low.astype(f32)).astype(bf16)


def tail(total_channels, got, proj_t, hid_t, steep, centred, inverse, conv, stream, packed):
    pieces, count = got.shape[0], stream.shape[0]
    channels = proj_t.shape[0]
    lane = lax.broadcasted_iota(jnp.int32, (32, 2 * channels), 1)
    hidden_grad = jnp.zeros((channels, count), f32)
    sums = jnp.zeros((16, count), f32)
    for j in range(pieces):
        part = got[j, :count, :]
        stream[:, j * LANES : (j + 1) * LANES] = part
        hidden_grad = hidden_grad + dot(proj_t[:, j * LANES : (j + 1) * LANES], part, NT)
        sums = sums + got[j, count : count + 16, :].astype(f32)
        outer = dot(part, hid_t[...], TN)
        for u in range(2):
            first = outer[64 * u : 64 * u + 32]
            second = outer[64 * u + 32 : 64 * u + 64]
            packed[2 * j + u] = jnp.where(lane < channels, first, second).astype(bf16)
    mean_one = (sums[0:1] + sums[1:2]) / total_channels
    mean_two = (sums[2:3] + sums[3:4]) / total_channels
    xhat = hidden_grad * steep[...]
    conv[...] = inverse[...] * (xhat - mean_one - centred[...] * mean_two)


def split_three(x):
    high = lax.reduce_precision(x, 8, 7)
    middle = lax.reduce_precision(x - high, 8, 7)
    return jnp.stack([high, middle, x - high - middle]).astype(bf16)


def norm_terms(conv, gain, mean, inverse):
    centred = (conv.astype(f32) - mean) * inverse
    normed = centred * gain
    sig = jax.nn.sigmoid(normed)
    steep = sig * (1.0 + normed * (1.0 - sig)) * gain
    return centred, normed * sig, steep


def body(
    stream_in,
    out_cot,
    route_experts,
    route_weights,
    w_gate,
    w_up,
    w_down,
    w_proj,
    conv_value,
    conv_gate,
    conv_taps,
    conv_result,
    channel_norm_gain,
):
    sp_count = lax.axis_size("sp")
    chips = lax.axis_size("chip")
    core = lax.axis_index("core")
    chip = lax.axis_index("chip")
    tp = 2 * chip + core
    tp_count = 2 * chips
    experts = w_gate.shape[0] * sp_count
    tokens, width = stream_in.shape
    top = route_experts.shape[1]
    capacity = 2 * top * tokens // experts
    share = capacity // 2
    rows = sp_count * share
    half = width // 2
    cols = width // tp_count
    hid = w_gate.shape[2]

    def halves(x, axis):
        shape = x.shape[:axis] + (chips, 2, cols) + x.shape[axis + 1 :]
        x = x.reshape(shape)
        mine = lax.dynamic_index_in_dim(x, core, axis + 1, keepdims=False)
        other = lax.dynamic_index_in_dim(x, 1 - core, axis + 1, keepdims=False)
        flat = shape[:axis] + (half,) + shape[axis + 3 :]
        return mine.reshape(flat), other.reshape(flat)

    w_own = jnp.stack([w_gate[0], w_up[0], w_down[0].T])
    w_own = jnp.concatenate(halves(w_own, 1), axis=1)
    w_far = swap_chips(w_own)

    ids = jnp.stack([core, chip % 2]).astype(jnp.int32)
    sent, slots = local_kernel(
        functools.partial(prepare, experts, capacity, share, chips),
        (shaped((experts * share, width), bf16), shaped((top, tokens), jnp.int32)),
        ids,
        route_experts.T,
        route_weights.T,
        stream_in,
        out_cot,
        specs=[SMEM, VMEM, VMEM, VMEM, VMEM],
    )
    mine = lax.all_to_all(sent.reshape(experts, share, width), "sp", 0, 0, tiled=True)
    mine = mine.reshape(rows, width)
    other = swap_cores(mine)

    act, gate_in, up_in, back_mine, back_other = local_kernel(
        experts_step,
        (
            shaped((rows, 2 * hid), bf16),
            shaped((rows, 2 * hid), bf16),
            shaped((rows, 2 * hid), bf16),
            shaped((rows, half), f32),
            shaped((rows, half), bf16),
        ),
        mine,
        other,
        w_own,
        w_far,
    )
    from_core = swap_cores(back_other)
    back = (back_mine + from_core.astype(f32)).astype(bf16)
    back = back.reshape(sp_count, share, chips, cols).transpose(0, 2, 1, 3)
    back = back.reshape(sp_count * chips, share, cols)
    back, act, gate_in, up_in = lax.optimization_barrier((back, act, gate_in, up_in))
    returned = lax.all_to_all(back, ("sp", "chip"), 0, 0, tiled=True)

    channels = conv_result.shape[0]
    channel_total = channels * tp_count
    positions = conv_result.shape[1]
    gains = jnp.pad(split_three(channel_norm_gain), ((0, 5), (0, positions - channels)))
    every = lax.all_gather(jnp.concatenate([conv_result, gains]), TP)
    all_conv = every[:, :channels].reshape(channel_total, positions).astype(f32)
    all_gain = jnp.sum(every[:, channels : channels + 3, :channels].astype(f32), axis=1)
    all_gain = all_gain.reshape(channel_total, 1)
    mean = jnp.sum(all_conv, axis=0) / channel_total
    variance = jnp.sum(all_conv * all_conv, axis=0) / channel_total - mean * mean
    inverse = lax.rsqrt(variance + norm_eps)
    all_centred, _, all_steep = norm_terms(all_conv, all_gain, mean, inverse)
    centred, hidden, steep = norm_terms(
        conv_result, channel_norm_gain[:, None], mean, inverse
    )
    hidden = hidden.astype(bf16)

    proj_t = w_proj.T
    proj_out = proj_t.reshape(channels, tp_count, cols).transpose(1, 0, 2)
    proj_out, mine_late = lax.optimization_barrier((proj_out, mine))
    proj_in = lax.all_to_all(proj_out, TP, 0, 0, tiled=True).reshape(channel_total, cols)
    lean_one = dot(all_steep.astype(bf16), proj_in, TN)
    lean_two = dot((all_steep * all_centred).astype(bf16), proj_in, TN)

    cot_cols = lax.dynamic_slice_in_dim(out_cot, tp * cols, cols, 1)
    payload = local_kernel(
        functools.partial(finish, capacity, share, chips),
        shaped((tokens + 16, cols), bf16),
        returned.reshape(experts * chips * share, cols),
        slots,
        cot_cols,
        lean_one,
        lean_two,
    )
    got = lax.all_gather(payload, TP)

    grad_conv, grad_stream, packed = local_kernel(
        functools.partial(tail, channel_total),
        (
            shaped((channels, positions), f32),
            shaped((tokens, width), bf16),
            shaped((sp_count, 32, 2 * channels), bf16),
        ),
        got,
        proj_t,
        jnp.concatenate([hidden, hidden]).T,
        steep,
        centred,
        inverse[None],
    )

    rows_in = jnp.concatenate([mine[:, :half], other[:, :half]], axis=1)
    cot_in = jnp.concatenate([mine[:, half:], other[:, half:]], axis=1)
    gate_far = dot(rows_in, gate_in[:, hid:], TN)
    up_far = dot(rows_in, up_in[:, hid:], TN)
    down_far = dot(act[:, hid:], cot_in, TN)
    far_in = swap_chips(jnp.stack([gate_far, up_far]).astype(bf16))
    down_far, packed = lax.optimization_barrier((down_far.astype(bf16), packed))
    far_down = swap_chips(down_far)
    gate_own = dot(rows_in, gate_in[:, :hid], TN) + far_in[0].astype(f32)
    up_own = dot(rows_in, up_in[:, :hid], TN) + far_in[1].astype(f32)
    down_own = dot(act[:, :hid], cot_in, TN) + far_down.astype(f32)

    def in_order(x, axis):
        shape = x.shape[:axis] + (2, chips, cols) + x.shape[axis + 1 :]
        x = x.astype(bf16).reshape(shape)
        x = jnp.where(core == 0, x, jnp.flip(x, axis))
        x = jnp.moveaxis(x, axis, axis + 1)
        return x.reshape(shape[:axis] + (width,) + shape[axis + 3 :])

    grad_gate = in_order(gate_own, 0)[None]
    grad_up = in_order(up_own, 0)[None]
    grad_down = in_order(down_own, 1)[None]

    packed = lax.all_to_all(packed, "sp", 0, 0, tiled=True)
    total = jnp.sum(packed.astype(f32), axis=0)
    grad_proj = jnp.concatenate([total[:, :channels], total[:, channels:]], axis=0)

    taps = conv_taps.shape[0]
    rim = lax.ppermute(
        grad_conv[:, : taps - 1], "sp", [(k, k - 1) for k in range(1, sp_count)]
    )
    extended = jnp.concatenate([grad_conv, rim], axis=1)
    grad_gated = jnp.zeros_like(grad_conv)
    for tap in range(taps):
        grad_gated = grad_gated + conv_taps[tap][:, None] * extended[:, tap : tap + positions]
    gate_sig = jax.nn.sigmoid(conv_gate.astype(f32))
    grad_value = (grad_gated * gate_sig).astype(bf16)
    grad_gate_in = (grad_gated * conv_value.astype(f32) * gate_sig * (1.0 - gate_sig)).astype(bf16)
    return (grad_gate, grad_up, grad_down, grad_stream, grad_proj, grad_value, grad_gate_in)


def solution(mesh):
    sp_count = mesh.shape["sp"]
    devices = mesh.devices.reshape(sp_count, -1, 2)
    return jax.shard_map(
        body,
        mesh=Mesh(devices, ("sp", "chip", "core")),
        in_specs=(
            P("sp", None),
            P("sp", None),
            P("sp", None),
            P("sp", None),
            P("sp", None, TP),
            P("sp", None, TP),
            P("sp", TP, None),
            P(None, TP),
            P(TP, "sp"),
            P(TP, "sp"),
            P(None, TP),
            P(TP, "sp"),
            P(TP),
        ),
        out_specs=(
            P("sp", None, TP),
            P("sp", None, TP),
            P("sp", TP, None),
            P("sp", None),
            P("sp", TP),
            P(TP, "sp"),
            P(TP, "sp"),
        ),
        check_vma=False,
    )
```

```python
import functools

import jax
import jax.numpy as jnp
from jax import lax
from jax.experimental import pallas as pl
from jax.experimental.pallas import tpu as pltpu
from jax.sharding import Mesh
from jax.sharding import PartitionSpec as P


norm_eps = 1e-05
clamp_limit = 7.0
alpha_gate = 1.702
bf16 = jnp.bfloat16
f32 = jnp.float32
LANES = 128


TP = ("chip", "core")
VMEM = pl.BlockSpec(memory_space=pltpu.VMEM)
SMEM = pl.BlockSpec(memory_space=pltpu.SMEM)


def dot(a, b, dims):
    return lax.dot_general(a, b, (dims, ((), ())), preferred_element_type=f32)


NN = ((1,), (0,))
NT = ((1,), (1,))
TN = ((0,), (0,))


def local_kernel(body, outs, *args, specs=None, flops=10**9):
    size = sum(a.size * a.dtype.itemsize for a in args)
    return pl.pallas_call(
        body,
        out_shape=outs,
        in_specs=[VMEM] * len(args) if specs is None else specs,
        out_specs=jax.tree.map(lambda _: VMEM, outs),
        cost_estimate=pl.CostEstimate(flops=flops, bytes_accessed=size, transcendentals=0),
        compiler_params=pltpu.CompilerParams(vmem_limit_bytes=40 * 2**20),
    )(*args)


def shaped(shape, dtype):
    return jax.ShapeDtypeStruct(shape, dtype)


def swap_cores(value):
    return lax.ppermute(value, "core", [(0, 1), (1, 0)])


def swap_chips(value):
    count = lax.axis_size("chip")
    return lax.ppermute(value, "chip", [(k, k ^ 1) for k in range(count)])


def prepare(experts, capacity, share, chips, ids, routes, weights, stream, cot, out, slots):
    top, count = routes.shape
    core, part = ids[0], ids[1]
    before = (
        lax.broadcasted_iota(jnp.int32, (count, count), 0)
        < lax.broadcasted_iota(jnp.int32, (count, count), 1)
    ).astype(bf16)
    named = lax.broadcasted_iota(jnp.int32, (experts, count), 0)
    row = lax.broadcasted_iota(jnp.int32, (experts * share, count), 0)
    base = jnp.zeros((experts, 1), f32)
    picked = jnp.zeros((experts * share, count), jnp.bool_)
    weight = jnp.zeros((experts * share, count), f32)
    for k in range(top):
        route = routes[k : k + 1, :]
        hot = named == route
        ones = jnp.where(hot, 1.0, 0.0)
        ahead = dot(ones.astype(bf16), before, NN) + base
        base = base + jnp.sum(ones, axis=1, keepdims=True)
        rank = jnp.sum(jnp.where(hot, ahead, 0.0), axis=0, keepdims=True).astype(jnp.int32)
        slots[k : k + 1, :] = route * capacity + rank
        local = rank - part * share
        held = (local >= 0) & (local < share)
        mine = row == jnp.where(held, route * share + local, -1)
        picked = picked | mine
        weight = weight + jnp.where(mine, weights[k : k + 1, :], 0.0)
    choice = jnp.where(picked, 1.0, 0.0).astype(bf16)
    scale = jnp.sum(weight, axis=1, keepdims=True)
    half = chips * LANES
    for i in range(chips):
        at = pl.ds(pl.multiple_of((2 * i + core) * LANES, LANES), LANES)
        out[:, i * LANES : (i + 1) * LANES] = dot(choice, stream[:, at], NN).astype(bf16)
        got = dot(choice, cot[:, at], NN)
        out[:, half + i * LANES : half + (i + 1) * LANES] = (scale * got).astype(bf16)


def experts_step(mine, other, own, far, own_acts, far_acts, back_mine, back_other):
    half = mine.shape[1] // 2
    for w, acts in ((own, own_acts), (far, far_acts)):

        def product(n, at):
            return dot(mine[:, at : at + half], w[n, :half], NN) + dot(
                other[:, at : at + half], w[n, half:], NN
            )

        pre_gate, pre_up, grad_act = product(0, 0), product(1, 0), product(2, half)
        glu = jnp.minimum(pre_gate, clamp_limit)
        lin = jnp.clip(pre_up, -clamp_limit, clamp_limit)
        sig = jax.nn.sigmoid(alpha_gate * glu)
        slope = sig + alpha_gate * glu * sig * (1.0 - sig)
        acts[2] = (glu * sig * (lin + 1.0)).astype(bf16)
        acts[0] = jnp.where(
            pre_gate < clamp_limit, grad_act * (lin + 1.0) * slope, 0.0
        ).astype(bf16)
        acts[1] = jnp.where(
            jnp.abs(pre_up) < clamp_limit, grad_act * glu * sig, 0.0
        ).astype(bf16)

    def back(at):
        total = 0.0
        for w, acts in ((own, own_acts), (far, far_acts)):
            total = total + dot(acts[0], w[0, at : at + half], NT)
            total = total + dot(acts[1], w[1, at : at + half], NT)
        return total

    back_other[...] = back(half).astype(bf16)
    back_mine[...] = back(0)


def weight_grads(chips, ids, mine, other, far, far_other, own_acts, far_acts, gate, up, down):
    core = ids[0]
    half = chips * LANES
    for turn, (near_rows, far_rows) in enumerate(((mine, far), (other, far_other))):
        which = core if turn == 0 else 1 - core
        for i in range(chips):
            at = pl.ds(pl.multiple_of((2 * i + which) * LANES, LANES), LANES)
            here = slice(i * LANES, (i + 1) * LANES)
            there = slice(half + i * LANES, half + (i + 1) * LANES)
            near, away = near_rows[:, here], far_rows[:, here]
            for n, out in enumerate((gate, up)):
                total = dot(near, own_acts[n], TN) + dot(away, far_acts[n], TN)
                out[at, :] = total.astype(bf16)
            total = dot(own_acts[2], near_rows[:, there], TN)
            total = total + dot(far_acts[2], far_rows[:, there], TN)
            down[:, at] = total.astype(bf16)


def finish(capacity, share, chips, data, slots, cot, lean_one, lean_two, out):
    rows, count = data.shape[0], slots.shape[1]
    row = lax.broadcasted_iota(jnp.int32, (rows, count), 0)
    expert = row // (chips * share)
    chip = (row // share) % chips
    key = expert * capacity + (chip % 2) * share + row % share
    hit = (key == slots[0:1, :]) | (key == slots[1:2, :])
    total = dot(jnp.where(hit, 1.0, 0.0).astype(bf16), data[...], TN)
    stream = (cot[...].astype(f32) + total).astype(bf16)
    out[0:count, :] = stream
    wide = stream.astype(f32)
    one = jnp.sum((wide * lean_one[...]).T, axis=0, keepdims=True)
    two = jnp.sum((wide * lean_two[...]).T, axis=0, keepdims=True)
    at = lax.broadcasted_iota(jnp.int32, (16, count), 0)
    both = jnp.where((at // 2) % 2 == 0, one, two)
    high = both.astype(bf16)
    low = (both - high.astype(f32)).astype(bf16)
    out[count : count + 16, :] = jnp.where(at % 2 == 0, high.astype(f32), low.astype(f32)).astype(bf16)


def tail(total_channels, got, proj_t, hid_t, steep, centred, inverse, conv, stream, packed):
    pieces, count = got.shape[0], stream.shape[0]
    channels = proj_t.shape[0]
    lane = lax.broadcasted_iota(jnp.int32, (32, 2 * channels), 1)
    hidden_grad = jnp.zeros((channels, count), f32)
    sums = jnp.zeros((16, count), f32)
    for j in range(pieces):
        part = got[j, :count, :]
        stream[:, j * LANES : (j + 1) * LANES] = part
        hidden_grad = hidden_grad + dot(proj_t[:, j * LANES : (j + 1) * LANES], part, NT)
        sums = sums + got[j, count : count + 16, :].astype(f32)
        outer = dot(part, hid_t[...], TN)
        for u in range(2):
            first = outer[64 * u : 64 * u + 32]
            second = outer[64 * u + 32 : 64 * u + 64]
            packed[2 * j + u] = jnp.where(lane < channels, first, second).astype(bf16)
    mean_one = (sums[0:1] + sums[1:2]) / total_channels
    mean_two = (sums[2:3] + sums[3:4]) / total_channels
    xhat = hidden_grad * steep[...]
    conv[...] = inverse[...] * (xhat - mean_one - centred[...] * mean_two)


def convolve(conv, rim, taps, gate, value, grad_value, grad_gate_in):
    count = conv.shape[1]
    lane = lax.broadcasted_iota(jnp.int32, conv.shape, 1)
    near, after = conv[...], rim[...]
    total = taps[:, 0:1] * near
    for tap in range(1, taps.shape[1]):
        shifted = jnp.where(
            lane < count - tap,
            pltpu.roll(near, count - tap, 1),
            pltpu.roll(after, count - tap, 1),
        )
        total = total + taps[:, tap : tap + 1] * shifted
    sig = jax.nn.sigmoid(gate[...].astype(f32))
    grad_value[...] = (total * sig).astype(bf16)
    grad_gate_in[...] = (total * value[...].astype(f32) * sig * (1.0 - sig)).astype(bf16)


def split_three(x):
    high = lax.reduce_precision(x, 8, 7)
    middle = lax.reduce_precision(x - high, 8, 7)
    return jnp.stack([high, middle, x - high - middle]).astype(bf16)


def norm_terms(conv, gain, mean, inverse):
    centred = (conv.astype(f32) - mean) * inverse
    normed = centred * gain
    sig = jax.nn.sigmoid(normed)
    steep = sig * (1.0 + normed * (1.0 - sig)) * gain
    return centred, normed * sig, steep


def body(
    stream_in,
    out_cot,
    route_experts,
    route_weights,
    w_gate,
    w_up,
    w_down,
    w_proj,
    conv_value,
    conv_gate,
    conv_taps,
    conv_result,
    channel_norm_gain,
):
    sp_count = lax.axis_size("sp")
    chips = lax.axis_size("chip")
    core = lax.axis_index("core")
    chip = lax.axis_index("chip")
    tp = 2 * chip + core
    tp_count = 2 * chips
    experts = w_gate.shape[0] * sp_count
    tokens, width = stream_in.shape
    top = route_experts.shape[1]
    capacity = 2 * top * tokens // experts
    share = capacity // 2
    rows = sp_count * share
    half = width // 2
    cols = width // tp_count
    hid = w_gate.shape[2]

    def halves(x, axis):
        shape = x.shape[:axis] + (chips, 2, cols) + x.shape[axis + 1 :]
        x = x.reshape(shape)
        mine = lax.dynamic_index_in_dim(x, core, axis + 1, keepdims=False)
        other = lax.dynamic_index_in_dim(x, 1 - core, axis + 1, keepdims=False)
        flat = shape[:axis] + (half,) + shape[axis + 3 :]
        return mine.reshape(flat), other.reshape(flat)

    channels = conv_result.shape[0]
    channel_total = channels * tp_count
    positions = conv_result.shape[1]
    proj_t = w_proj.T
    proj_out = proj_t.reshape(channels, tp_count, cols).transpose(1, 0, 2)
    proj_in = lax.all_to_all(proj_out, TP, 0, 0, tiled=True)

    w_own = jnp.stack([w_gate[0], w_up[0], w_down[0].T])
    w_own = jnp.concatenate(halves(w_own, 1), axis=1)
    w_far = swap_chips(w_own)

    ids = jnp.stack([core, chip % 2]).astype(jnp.int32)
    sent, slots = local_kernel(
        functools.partial(prepare, experts, capacity, share, chips),
        (shaped((experts * share, width), bf16), shaped((top, tokens), jnp.int32)),
        ids,
        route_experts.T,
        route_weights.T,
        stream_in,
        out_cot,
        specs=[SMEM, VMEM, VMEM, VMEM, VMEM],
    )
    sent, proj_in, w_own = lax.optimization_barrier((sent, proj_in, w_own))
    mine = lax.all_to_all(sent.reshape(experts, share, width), "sp", 0, 0, tiled=True)
    mine = mine.reshape(rows, width)
    other = swap_cores(mine)

    far_rows = swap_chips(mine)

    own_acts, far_acts, back_mine, back_other = local_kernel(
        experts_step,
        (
            shaped((3, rows, hid), bf16),
            shaped((3, rows, hid), bf16),
            shaped((rows, half), f32),
            shaped((rows, half), bf16),
        ),
        mine,
        other,
        w_own,
        w_far,
    )
    from_core = swap_cores(back_other)
    back = (back_mine + from_core.astype(f32)).astype(bf16)
    back = back.reshape(sp_count, share, chips, cols).transpose(0, 2, 1, 3)
    back = back.reshape(sp_count * chips, share, cols)
    gains = jnp.pad(split_three(channel_norm_gain), ((0, 5), (0, positions - channels)))
    conv_out = jnp.concatenate([conv_result, gains])
    back, own_acts, far_acts, conv_out = lax.optimization_barrier(
        (back, own_acts, far_acts, conv_out)
    )
    returned = lax.all_to_all(back, ("sp", "chip"), 0, 0, tiled=True)

    far_acts = swap_chips(far_acts)
    far_other = swap_cores(far_rows)
    gate, up, down = local_kernel(
        functools.partial(weight_grads, chips),
        (shaped((width, hid), bf16), shaped((width, hid), bf16), shaped((hid, width), bf16)),
        ids,
        mine,
        other,
        far_rows,
        far_other,
        own_acts,
        far_acts,
        specs=[SMEM] + [VMEM] * 6,
    )
    grad_gate, grad_up, grad_down = gate[None], up[None], down[None]

    every = lax.all_gather(conv_out, TP)
    all_conv = every[:, :channels].reshape(channel_total, positions).astype(f32)
    all_gain = jnp.sum(every[:, channels : channels + 3, :channels].astype(f32), axis=1)
    all_gain = all_gain.reshape(channel_total, 1)
    mean = jnp.sum(all_conv, axis=0) / channel_total
    variance = jnp.sum(all_conv * all_conv, axis=0) / channel_total - mean * mean
    inverse = lax.rsqrt(variance + norm_eps)
    all_centred, _, all_steep = norm_terms(all_conv, all_gain, mean, inverse)
    centred, hidden, steep = norm_terms(
        conv_result, channel_norm_gain[:, None], mean, inverse
    )
    hidden = hidden.astype(bf16)

    proj_in = proj_in.reshape(channel_total, cols)
    lean_one = dot(all_steep.astype(bf16), proj_in, TN)
    lean_two = dot((all_steep * all_centred).astype(bf16), proj_in, TN)

    cot_cols = lax.dynamic_slice_in_dim(out_cot, tp * cols, cols, 1)
    payload = local_kernel(
        functools.partial(finish, capacity, share, chips),
        shaped((tokens + 16, cols), bf16),
        returned.reshape(experts * chips * share, cols),
        slots,
        cot_cols,
        lean_one,
        lean_two,
    )
    got = lax.all_gather(payload, TP)

    grad_conv, grad_stream, packed = local_kernel(
        functools.partial(tail, channel_total),
        (
            shaped((channels, positions), f32),
            shaped((tokens, width), bf16),
            shaped((sp_count, 32, 2 * channels), bf16),
        ),
        got,
        proj_t,
        jnp.concatenate([hidden, hidden]).T,
        steep,
        centred,
        inverse[None],
    )

    packed = lax.all_to_all(packed, "sp", 0, 0, tiled=True)
    total = jnp.sum(packed.astype(f32), axis=0)
    grad_proj = jnp.concatenate([total[:, :channels], total[:, channels:]], axis=0)

    rim = lax.ppermute(grad_conv, "sp", [(k, k - 1) for k in range(1, sp_count)])
    grad_value, grad_gate_in = local_kernel(
        convolve,
        (shaped((channels, positions), bf16), shaped((channels, positions), bf16)),
        grad_conv,
        rim,
        conv_taps.T,
        conv_gate,
        conv_value,
    )
    return (grad_gate, grad_up, grad_down, grad_stream, grad_proj, grad_value, grad_gate_in)


def solution(mesh):
    sp_count = mesh.shape["sp"]
    devices = mesh.devices.reshape(sp_count, -1, 2)
    return jax.shard_map(
        body,
        mesh=Mesh(devices, ("sp", "chip", "core")),
        in_specs=(
            P("sp", None),
            P("sp", None),
            P("sp", None),
            P("sp", None),
            P("sp", None, TP),
            P("sp", None, TP),
            P("sp", TP, None),
            P(None, TP),
            P(TP, "sp"),
            P(TP, "sp"),
            P(None, TP),
            P(TP, "sp"),
            P(TP),
        ),
        out_specs=(
            P("sp", None, TP),
            P("sp", None, TP),
            P("sp", TP, None),
            P("sp", None),
            P("sp", TP),
            P(TP, "sp"),
            P(TP, "sp"),
        ),
        check_vma=False,
    )
```

```python
import functools

import jax
import jax.numpy as jnp
from jax import lax
from jax.experimental import pallas as pl
from jax.experimental.pallas import tpu as pltpu
from jax.sharding import Mesh
from jax.sharding import PartitionSpec as P


norm_eps = 1e-05
clamp_limit = 7.0
alpha_gate = 1.702
bf16 = jnp.bfloat16
f32 = jnp.float32
LANES = 128


TP = ("chip", "core")
VMEM = pl.BlockSpec(memory_space=pltpu.VMEM)
SMEM = pl.BlockSpec(memory_space=pltpu.SMEM)


def dot(a, b, dims):
    return lax.dot_general(a, b, (dims, ((), ())), preferred_element_type=f32)


NN = ((1,), (0,))
NT = ((1,), (1,))
TN = ((0,), (0,))


def local_kernel(body, outs, *args, specs=None, flops=10**9):
    size = sum(a.size * a.dtype.itemsize for a in args)
    return pl.pallas_call(
        body,
        out_shape=outs,
        in_specs=[VMEM] * len(args) if specs is None else specs,
        out_specs=jax.tree.map(lambda _: VMEM, outs),
        cost_estimate=pl.CostEstimate(flops=flops, bytes_accessed=size, transcendentals=0),
        compiler_params=pltpu.CompilerParams(vmem_limit_bytes=40 * 2**20),
    )(*args)


def shaped(shape, dtype):
    return jax.ShapeDtypeStruct(shape, dtype)


def swap_cores(value):
    return lax.ppermute(value, "core", [(0, 1), (1, 0)])


def swap_chips(value):
    count = lax.axis_size("chip")
    return lax.ppermute(value, "chip", [(k, k ^ 1) for k in range(count)])


def prepare(experts, capacity, share, chips, ids, routes, weights, stream, cot, out, slots):
    top, count = routes.shape
    core, part = ids[0], ids[1]
    before = (
        lax.broadcasted_iota(jnp.int32, (count, count), 0)
        < lax.broadcasted_iota(jnp.int32, (count, count), 1)
    ).astype(bf16)
    named = lax.broadcasted_iota(jnp.int32, (experts, count), 0)
    row = lax.broadcasted_iota(jnp.int32, (experts * share, count), 0)
    base = jnp.zeros((experts, 1), f32)
    picked = jnp.zeros((experts * share, count), jnp.bool_)
    weight = jnp.zeros((experts * share, count), f32)
    for k in range(top):
        route = routes[k : k + 1, :]
        hot = named == route
        ones = jnp.where(hot, 1.0, 0.0)
        ahead = dot(ones.astype(bf16), before, NN) + base
        base = base + jnp.sum(ones, axis=1, keepdims=True)
        rank = jnp.sum(jnp.where(hot, ahead, 0.0), axis=0, keepdims=True).astype(jnp.int32)
        slots[k : k + 1, :] = route * capacity + rank
        local = rank - part * share
        held = (local >= 0) & (local < share)
        mine = row == jnp.where(held, route * share + local, -1)
        picked = picked | mine
        weight = weight + jnp.where(mine, weights[k : k + 1, :], 0.0)
    choice = jnp.where(picked, 1.0, 0.0).astype(bf16)
    scale = jnp.sum(weight, axis=1, keepdims=True)
    half = chips * LANES
    for i in range(chips):
        at = pl.ds(pl.multiple_of((2 * i + core) * LANES, LANES), LANES)
        out[:, i * LANES : (i + 1) * LANES] = dot(choice, stream[:, at], NN).astype(bf16)
        got = dot(choice, cot[:, at], NN)
        out[:, half + i * LANES : half + (i + 1) * LANES] = (scale * got).astype(bf16)


def experts_step(mine, other, own, far, own_acts, far_acts, back_mine, back_other):
    half = mine.shape[1] // 2
    for w, acts in ((own, own_acts), (far, far_acts)):

        def product(n, at):
            return dot(mine[:, at : at + half], w[n, :half], NN) + dot(
                other[:, at : at + half], w[n, half:], NN
            )

        pre_gate, pre_up, grad_act = product(0, 0), product(1, 0), product(2, half)
        glu = jnp.minimum(pre_gate, clamp_limit)
        lin = jnp.clip(pre_up, -clamp_limit, clamp_limit)
        sig = jax.nn.sigmoid(alpha_gate * glu)
        slope = sig + alpha_gate * glu * sig * (1.0 - sig)
        acts[2] = (glu * sig * (lin + 1.0)).astype(bf16)
        acts[0] = jnp.where(
            pre_gate < clamp_limit, grad_act * (lin + 1.0) * slope, 0.0
        ).astype(bf16)
        acts[1] = jnp.where(
            jnp.abs(pre_up) < clamp_limit, grad_act * glu * sig, 0.0
        ).astype(bf16)

    def back(at):
        total = 0.0
        for w, acts in ((own, own_acts), (far, far_acts)):
            total = total + dot(acts[0], w[0, at : at + half], NT)
            total = total + dot(acts[1], w[1, at : at + half], NT)
        return total

    back_other[...] = back(half).astype(bf16)
    back_mine[...] = back(0)


def weight_grads(chips, ids, mine, other, far, far_other, own_acts, far_acts, gate, up, down):
    core = ids[0]
    half = chips * LANES
    for turn, (near_rows, far_rows) in enumerate(((mine, far), (other, far_other))):
        which = core if turn == 0 else 1 - core
        for i in range(chips):
            at = pl.ds(pl.multiple_of((2 * i + which) * LANES, LANES), LANES)
            here = slice(i * LANES, (i + 1) * LANES)
            there = slice(half + i * LANES, half + (i + 1) * LANES)
            near, away = near_rows[:, here], far_rows[:, here]
            for n, out in enumerate((gate, up)):
                total = dot(near, own_acts[n], TN) + dot(away, far_acts[n], TN)
                out[at, :] = total.astype(bf16)
            total = dot(own_acts[2], near_rows[:, there], TN)
            total = total + dot(far_acts[2], far_rows[:, there], TN)
            down[:, at] = total.astype(bf16)


def finish(capacity, share, chips, data, slots, cot, lean_one, lean_two, out):
    rows, count = data.shape[0], slots.shape[1]
    row = lax.broadcasted_iota(jnp.int32, (rows, count), 0)
    expert = row // (chips * share)
    chip = (row // share) % chips
    key = expert * capacity + (chip % 2) * share + row % share
    hit = (key == slots[0:1, :]) | (key == slots[1:2, :])
    total = dot(jnp.where(hit, 1.0, 0.0).astype(bf16), data[...], TN)
    stream = (cot[...].astype(f32) + total).astype(bf16)
    out[0:count, :] = stream
    wide = stream.astype(f32)
    one = jnp.sum((wide * lean_one[...]).T, axis=0, keepdims=True)
    two = jnp.sum((wide * lean_two[...]).T, axis=0, keepdims=True)
    at = lax.broadcasted_iota(jnp.int32, (16, count), 0)
    both = jnp.where((at // 2) % 2 == 0, one, two)
    high = both.astype(bf16)
    low = (both - high.astype(f32)).astype(bf16)
    out[count : count + 16, :] = jnp.where(at % 2 == 0, high.astype(f32), low.astype(f32)).astype(bf16)


def tail(total_channels, got, proj_t, hid_t, steep, centred, inverse, conv, stream, packed):
    pieces, count = got.shape[0], stream.shape[0]
    channels = proj_t.shape[0]
    lane = lax.broadcasted_iota(jnp.int32, (32, 2 * channels), 1)
    hidden_grad = jnp.zeros((channels, count), f32)
    sums = jnp.zeros((16, count), f32)
    for j in range(pieces):
        part = got[j, :count, :]
        stream[:, j * LANES : (j + 1) * LANES] = part
        hidden_grad = hidden_grad + dot(proj_t[:, j * LANES : (j + 1) * LANES], part, NT)
        sums = sums + got[j, count : count + 16, :].astype(f32)
        outer = dot(part, hid_t[...], TN)
        for u in range(2):
            first = outer[64 * u : 64 * u + 32]
            second = outer[64 * u + 32 : 64 * u + 64]
            packed[2 * j + u] = jnp.where(lane < channels, first, second).astype(bf16)
    mean_one = (sums[0:1] + sums[1:2]) / total_channels
    mean_two = (sums[2:3] + sums[3:4]) / total_channels
    xhat = hidden_grad * steep[...]
    conv[...] = inverse[...] * (xhat - mean_one - centred[...] * mean_two)


def convolve(conv, rim, taps, gate, value, grad_value, grad_gate_in):
    count = conv.shape[1]
    lane = lax.broadcasted_iota(jnp.int32, conv.shape, 1)
    near, after = conv[...], rim[...]
    total = taps[:, 0:1] * near
    for tap in range(1, taps.shape[1]):
        shifted = jnp.where(
            lane < count - tap,
            pltpu.roll(near, count - tap, 1),
            pltpu.roll(after, count - tap, 1),
        )
        total = total + taps[:, tap : tap + 1] * shifted
    sig = jax.nn.sigmoid(gate[...].astype(f32))
    grad_value[...] = (total * sig).astype(bf16)
    grad_gate_in[...] = (total * value[...].astype(f32) * sig * (1.0 - sig)).astype(bf16)


def split_three(x):
    high = lax.reduce_precision(x, 8, 7)
    middle = lax.reduce_precision(x - high, 8, 7)
    return jnp.stack([high, middle, x - high - middle]).astype(bf16)


def norm_terms(conv, gain, mean, inverse):
    centred = (conv.astype(f32) - mean) * inverse
    normed = centred * gain
    sig = jax.nn.sigmoid(normed)
    steep = sig * (1.0 + normed * (1.0 - sig)) * gain
    return centred, normed * sig, steep


def body(
    stream_in,
    out_cot,
    route_experts,
    route_weights,
    w_gate,
    w_up,
    w_down,
    w_proj,
    conv_value,
    conv_gate,
    conv_taps,
    conv_result,
    channel_norm_gain,
):
    sp_count = lax.axis_size("sp")
    chips = lax.axis_size("chip")
    core = lax.axis_index("core")
    chip = lax.axis_index("chip")
    tp = 2 * chip + core
    tp_count = 2 * chips
    experts = w_gate.shape[0] * sp_count
    tokens, width = stream_in.shape
    top = route_experts.shape[1]
    capacity = 2 * top * tokens // experts
    share = capacity // 2
    rows = sp_count * share
    half = width // 2
    cols = width // tp_count
    hid = w_gate.shape[2]

    def halves(x, axis):
        shape = x.shape[:axis] + (chips, 2, cols) + x.shape[axis + 1 :]
        x = x.reshape(shape)
        mine = lax.dynamic_index_in_dim(x, core, axis + 1, keepdims=False)
        other = lax.dynamic_index_in_dim(x, 1 - core, axis + 1, keepdims=False)
        flat = shape[:axis] + (half,) + shape[axis + 3 :]
        return mine.reshape(flat), other.reshape(flat)

    channels = conv_result.shape[0]
    channel_total = channels * tp_count
    positions = conv_result.shape[1]
    proj_t = w_proj.T
    gains = jnp.pad(split_three(channel_norm_gain), ((0, 5), (0, positions - channels)))
    shared = jnp.concatenate([conv_result, gains])
    proj_out = jnp.concatenate(
        [
            proj_t.reshape(channels, tp_count, cols).transpose(1, 0, 2),
            jnp.broadcast_to(shared, (tp_count, *shared.shape)),
        ],
        axis=1,
    )

    w_own = jnp.stack([w_gate[0], w_up[0], w_down[0].T])
    w_own = jnp.concatenate(halves(w_own, 1), axis=1)
    w_far = swap_chips(w_own)

    ids = jnp.stack([core, chip % 2]).astype(jnp.int32)
    sent, slots = local_kernel(
        functools.partial(prepare, experts, capacity, share, chips),
        (shaped((experts * share, width), bf16), shaped((top, tokens), jnp.int32)),
        ids,
        route_experts.T,
        route_weights.T,
        stream_in,
        out_cot,
        specs=[SMEM, VMEM, VMEM, VMEM, VMEM],
    )
    mine = lax.all_to_all(sent.reshape(experts, share, width), "sp", 0, 0, tiled=True)
    mine = mine.reshape(rows, width)
    other = swap_cores(mine)
    proj_out, _ = lax.optimization_barrier((proj_out, mine))
    every = lax.all_to_all(proj_out, TP, 0, 0, tiled=True)

    far_rows = swap_chips(mine)

    own_acts, far_acts, back_mine, back_other = local_kernel(
        experts_step,
        (
            shaped((3, rows, hid), bf16),
            shaped((3, rows, hid), bf16),
            shaped((rows, half), f32),
            shaped((rows, half), bf16),
        ),
        mine,
        other,
        w_own,
        w_far,
    )
    from_core = swap_cores(back_other)
    back = (back_mine + from_core.astype(f32)).astype(bf16)
    back = back.reshape(sp_count, share, chips, cols).transpose(0, 2, 1, 3)
    back = back.reshape(sp_count * chips, share, cols)
    back, own_acts, far_acts, every = lax.optimization_barrier(
        (back, own_acts, far_acts, every)
    )
    returned = lax.all_to_all(back, ("sp", "chip"), 0, 0, tiled=True)

    far_acts = swap_chips(far_acts)
    proj_in = every[:, :channels].reshape(channel_total, cols)
    every = every[:, channels:]
    all_conv = every[:, :channels].reshape(channel_total, positions).astype(f32)
    all_gain = jnp.sum(every[:, channels : channels + 3, :channels].astype(f32), axis=1)
    all_gain = all_gain.reshape(channel_total, 1)
    mean = jnp.sum(all_conv, axis=0) / channel_total
    variance = jnp.sum(all_conv * all_conv, axis=0) / channel_total - mean * mean
    inverse = lax.rsqrt(variance + norm_eps)
    all_centred, _, all_steep = norm_terms(all_conv, all_gain, mean, inverse)
    centred, hidden, steep = norm_terms(
        conv_result, channel_norm_gain[:, None], mean, inverse
    )
    hidden = hidden.astype(bf16)

    lean_one = dot(all_steep.astype(bf16), proj_in, TN)
    lean_two = dot((all_steep * all_centred).astype(bf16), proj_in, TN)

    cot_cols = lax.dynamic_slice_in_dim(out_cot, tp * cols, cols, 1)
    payload = local_kernel(
        functools.partial(finish, capacity, share, chips),
        shaped((tokens + 16, cols), bf16),
        returned.reshape(experts * chips * share, cols),
        slots,
        cot_cols,
        lean_one,
        lean_two,
    )
    got = lax.all_gather(payload, TP)
    far_rows, _ = lax.optimization_barrier((far_rows, got))
    far_other = swap_cores(far_rows)
    gate, up, down = local_kernel(
        functools.partial(weight_grads, chips),
        (shaped((width, hid), bf16), shaped((width, hid), bf16), shaped((hid, width), bf16)),
        ids,
        mine,
        other,
        far_rows,
        far_other,
        own_acts,
        far_acts,
        specs=[SMEM] + [VMEM] * 6,
    )
    grad_gate, grad_up, grad_down = gate[None], up[None], down[None]


    grad_conv, grad_stream, packed = local_kernel(
        functools.partial(tail, channel_total),
        (
            shaped((channels, positions), f32),
            shaped((tokens, width), bf16),
            shaped((sp_count, 32, 2 * channels), bf16),
        ),
        got,
        proj_t,
        jnp.concatenate([hidden, hidden]).T,
        steep,
        centred,
        inverse[None],
    )

    packed = lax.all_to_all(packed, "sp", 0, 0, tiled=True)
    total = jnp.sum(packed.astype(f32), axis=0)
    grad_proj = jnp.concatenate([total[:, :channels], total[:, channels:]], axis=0)

    rim = lax.ppermute(grad_conv, "sp", [(k, k - 1) for k in range(1, sp_count)])
    grad_value, grad_gate_in = local_kernel(
        convolve,
        (shaped((channels, positions), bf16), shaped((channels, positions), bf16)),
        grad_conv,
        rim,
        conv_taps.T,
        conv_gate,
        conv_value,
    )
    return (grad_gate, grad_up, grad_down, grad_stream, grad_proj, grad_value, grad_gate_in)


def solution(mesh):
    sp_count = mesh.shape["sp"]
    devices = mesh.devices.reshape(sp_count, -1, 2)
    return jax.shard_map(
        body,
        mesh=Mesh(devices, ("sp", "chip", "core")),
        in_specs=(
            P("sp", None),
            P("sp", None),
            P("sp", None),
            P("sp", None),
            P("sp", None, TP),
            P("sp", None, TP),
            P("sp", TP, None),
            P(None, TP),
            P(TP, "sp"),
            P(TP, "sp"),
            P(None, TP),
            P(TP, "sp"),
            P(TP),
        ),
        out_specs=(
            P("sp", None, TP),
            P("sp", None, TP),
            P("sp", TP, None),
            P("sp", None),
            P("sp", TP),
            P(TP, "sp"),
            P(TP, "sp"),
        ),
        check_vma=False,
    )
```

```python
import functools

import jax
import jax.numpy as jnp
from jax import lax
from jax.experimental import pallas as pl
from jax.experimental.pallas import tpu as pltpu
from jax.sharding import Mesh
from jax.sharding import PartitionSpec as P


norm_eps = 1e-05
clamp_limit = 7.0
alpha_gate = 1.702
bf16 = jnp.bfloat16
f32 = jnp.float32
LANES = 128


TP = ("chip", "core")
VMEM = pl.BlockSpec(memory_space=pltpu.VMEM)
SMEM = pl.BlockSpec(memory_space=pltpu.SMEM)


def dot(a, b, dims):
    return lax.dot_general(a, b, (dims, ((), ())), preferred_element_type=f32)


NN = ((1,), (0,))
NT = ((1,), (1,))
TN = ((0,), (0,))


def local_kernel(body, outs, *args, specs=None, flops=10**9):
    size = sum(a.size * a.dtype.itemsize for a in args)
    return pl.pallas_call(
        body,
        out_shape=outs,
        in_specs=[VMEM] * len(args) if specs is None else specs,
        out_specs=jax.tree.map(lambda _: VMEM, outs),
        cost_estimate=pl.CostEstimate(flops=flops, bytes_accessed=size, transcendentals=0),
        compiler_params=pltpu.CompilerParams(vmem_limit_bytes=40 * 2**20),
    )(*args)


def shaped(shape, dtype):
    return jax.ShapeDtypeStruct(shape, dtype)


def swap_cores(value):
    return lax.ppermute(value, "core", [(0, 1), (1, 0)])


def swap_chips(value):
    count = lax.axis_size("chip")
    return lax.ppermute(value, "chip", [(k, k ^ 1) for k in range(count)])


def pack_weights(chips, ids, gate, up, down, out):
    half = chips * LANES
    for turn in range(2):
        which = ids[0] if turn == 0 else 1 - ids[0]
        for i in range(chips):
            at = pl.ds(pl.multiple_of((2 * i + which) * LANES, LANES), LANES)
            here = slice(turn * half + i * LANES, turn * half + (i + 1) * LANES)
            out[0, here, :] = gate[at, :]
            out[1, here, :] = up[at, :]
            out[2, here, :] = down[:, at]


def prepare(experts, capacity, share, chips, ids, routes, weights, stream, cot, out, slots):
    top, count = routes.shape
    core, part = ids[0], ids[1]
    before = (
        lax.broadcasted_iota(jnp.int32, (count, count), 0)
        < lax.broadcasted_iota(jnp.int32, (count, count), 1)
    ).astype(bf16)
    named = lax.broadcasted_iota(jnp.int32, (experts, count), 0)
    row = lax.broadcasted_iota(jnp.int32, (experts * share, count), 0)
    base = jnp.zeros((experts, 1), f32)
    picked = jnp.zeros((experts * share, count), jnp.bool_)
    weight = jnp.zeros((experts * share, count), f32)
    for k in range(top):
        route = routes[k : k + 1, :]
        hot = named == route
        ones = jnp.where(hot, 1.0, 0.0)
        ahead = dot(ones.astype(bf16), before, NN) + base
        base = base + jnp.sum(ones, axis=1, keepdims=True)
        rank = jnp.sum(jnp.where(hot, ahead, 0.0), axis=0, keepdims=True).astype(jnp.int32)
        slots[k : k + 1, :] = route * capacity + rank
        local = rank - part * share
        held = (local >= 0) & (local < share)
        mine = row == jnp.where(held, route * share + local, -1)
        picked = picked | mine
        weight = weight + jnp.where(mine, weights[k : k + 1, :], 0.0)
    choice = jnp.where(picked, 1.0, 0.0).astype(bf16)
    scale = jnp.sum(weight, axis=1, keepdims=True)
    half = chips * LANES
    for i in range(chips):
        at = pl.ds(pl.multiple_of((2 * i + core) * LANES, LANES), LANES)
        out[:, i * LANES : (i + 1) * LANES] = dot(choice, stream[:, at], NN).astype(bf16)
        got = dot(choice, cot[:, at], NN)
        out[:, half + i * LANES : half + (i + 1) * LANES] = (scale * got).astype(bf16)


def experts_step(mine, other, own, far, own_acts, far_acts, back_mine, back_other):
    half = mine.shape[1] // 2
    for w, acts in ((own, own_acts), (far, far_acts)):

        def product(n, at):
            return dot(mine[:, at : at + half], w[n, :half], NN) + dot(
                other[:, at : at + half], w[n, half:], NN
            )

        pre_gate, pre_up = product(0, 0), product(1, 0)
        grad_act = 0.0
        for i in range(half // LANES):
            here, there = i * LANES, half + i * LANES
            block = slice(there, there + LANES)
            grad_act = grad_act + dot(mine[:, block], w[2, here : here + LANES], NT)
            grad_act = grad_act + dot(other[:, block], w[2, there : there + LANES], NT)
        glu = jnp.minimum(pre_gate, clamp_limit)
        lin = jnp.clip(pre_up, -clamp_limit, clamp_limit)
        sig = jax.nn.sigmoid(alpha_gate * glu)
        slope = sig + alpha_gate * glu * sig * (1.0 - sig)
        acts[2] = (glu * sig * (lin + 1.0)).astype(bf16)
        acts[0] = jnp.where(
            pre_gate < clamp_limit, grad_act * (lin + 1.0) * slope, 0.0
        ).astype(bf16)
        acts[1] = jnp.where(
            jnp.abs(pre_up) < clamp_limit, grad_act * glu * sig, 0.0
        ).astype(bf16)

    def back(at):
        total = 0.0
        for w, acts in ((own, own_acts), (far, far_acts)):
            total = total + dot(acts[0], w[0, at : at + half], NT)
            total = total + dot(acts[1], w[1, at : at + half], NT)
        return total

    back_other[...] = back(half).astype(bf16)
    back_mine[...] = back(0)


def weight_grads(chips, ids, mine, other, far, far_other, own_acts, far_acts, gate, up, down):
    core = ids[0]
    half = chips * LANES
    for turn, (near_rows, far_rows) in enumerate(((mine, far), (other, far_other))):
        which = core if turn == 0 else 1 - core
        for i in range(chips):
            at = pl.ds(pl.multiple_of((2 * i + which) * LANES, LANES), LANES)
            here = slice(i * LANES, (i + 1) * LANES)
            there = slice(half + i * LANES, half + (i + 1) * LANES)
            near, away = near_rows[:, here], far_rows[:, here]
            for n, out in enumerate((gate, up)):
                total = dot(near, own_acts[n], TN) + dot(away, far_acts[n], TN)
                out[at, :] = total.astype(bf16)
            total = dot(own_acts[2], near_rows[:, there], TN)
            total = total + dot(far_acts[2], far_rows[:, there], TN)
            down[:, at] = total.astype(bf16)


def in_parts(x):
    high = x.astype(bf16).astype(f32)
    middle = (x - high).astype(bf16).astype(f32)
    return high, middle, x - high - middle


def finish(capacity, share, chips, data, slots, cot, conv, out):
    rows, count = data.shape[0], slots.shape[1]
    row = lax.broadcasted_iota(jnp.int32, (rows, count), 0)
    expert = row // (chips * share)
    chip = (row // share) % chips
    key = expert * capacity + (chip % 2) * share + row % share
    hit = (key == slots[0:1, :]) | (key == slots[1:2, :])
    total = dot(jnp.where(hit, 1.0, 0.0).astype(bf16), data[...], TN)
    out[0:count, :] = (cot[...].astype(f32) + total).astype(bf16)
    wide = conv[...].astype(f32)
    at = lax.broadcasted_iota(jnp.int32, (16, count), 0)
    block = jnp.zeros((16, count), f32)
    sums = jnp.sum(wide, axis=0, keepdims=True), jnp.sum(wide * wide, axis=0, keepdims=True)
    for n, x in enumerate(in_parts(sums[0]) + in_parts(sums[1])):
        block = jnp.where(at == n, x, block)
    out[count : count + 16, :] = block.astype(bf16)


def tail(total_channels, got, proj_t, conv, gain, xhat, centred, inverse, sums, stream, packed):
    pieces, count = got.shape[0], stream.shape[0]
    channels = proj_t.shape[0]
    lane = lax.broadcasted_iota(jnp.int32, (32, 2 * channels), 1)
    parts = jnp.zeros((16, count), f32)
    for j in range(pieces):
        parts = parts + got[j, count : count + 16, :].astype(f32)
    mean = (parts[0:1] + parts[1:2] + parts[2:3]) / total_channels
    square = (parts[3:4] + parts[4:5] + parts[5:6]) / total_channels
    scale = lax.rsqrt(square - mean * mean + norm_eps)
    removed = (conv[...].astype(f32) - mean) * scale
    normed = removed * gain[...]
    sig = jax.nn.sigmoid(normed)
    hidden = normed * sig
    hid_t = jnp.concatenate([hidden, hidden]).T.astype(bf16)
    hidden_grad = jnp.zeros((channels, count), f32)
    for j in range(pieces):
        part = got[j, :count, :]
        stream[:, j * LANES : (j + 1) * LANES] = part
        hidden_grad = hidden_grad + dot(proj_t[:, j * LANES : (j + 1) * LANES], part, NT)
        outer = dot(part, hid_t, TN)
        for u in range(2):
            first = outer[64 * u : 64 * u + 32]
            second = outer[64 * u + 32 : 64 * u + 64]
            packed[2 * j + u] = jnp.where(lane < channels, first, second).astype(bf16)
    grown = hidden_grad * sig * (1.0 + normed * (1.0 - sig)) * gain[...]
    xhat[...] = grown
    centred[...] = removed
    inverse[...] = scale
    at = lax.broadcasted_iota(jnp.int32, (8, count), 0)
    one = jnp.sum(grown, axis=0, keepdims=True)
    two = jnp.sum(grown * removed, axis=0, keepdims=True)
    block = jnp.where(at == 0, one, jnp.where(at == 1, two, 0.0))
    for j in range(pieces):
        sums[j] = block


def normalise(total_channels, sums, xhat, centred, inverse, conv):
    block = jnp.zeros(sums.shape[1:], f32)
    for j in range(sums.shape[0]):
        block = block + sums[j]
    block = block / total_channels
    conv[...] = inverse[...] * (xhat[...] - block[0:1] - centred[...] * block[1:2])


def convolve(conv, rim, taps, gate, value, grad_value, grad_gate_in):
    count = conv.shape[1]
    lane = lax.broadcasted_iota(jnp.int32, conv.shape, 1)
    near, after = conv[...], rim[...]
    total = taps[:, 0:1] * near
    for tap in range(1, taps.shape[1]):
        shifted = jnp.where(
            lane < count - tap,
            pltpu.roll(near, count - tap, 1),
            pltpu.roll(after, count - tap, 1),
        )
        total = total + taps[:, tap : tap + 1] * shifted
    sig = jax.nn.sigmoid(gate[...].astype(f32))
    grad_value[...] = (total * sig).astype(bf16)
    grad_gate_in[...] = (total * value[...].astype(f32) * sig * (1.0 - sig)).astype(bf16)


def body(
    stream_in,
    out_cot,
    route_experts,
    route_weights,
    w_gate,
    w_up,
    w_down,
    w_proj,
    conv_value,
    conv_gate,
    conv_taps,
    conv_result,
    channel_norm_gain,
):
    sp_count = lax.axis_size("sp")
    chips = lax.axis_size("chip")
    core = lax.axis_index("core")
    chip = lax.axis_index("chip")
    tp = 2 * chip + core
    tp_count = 2 * chips
    experts = w_gate.shape[0] * sp_count
    tokens, width = stream_in.shape
    top = route_experts.shape[1]
    capacity = 2 * top * tokens // experts
    share = capacity // 2
    rows = sp_count * share
    half = width // 2
    cols = width // tp_count
    hid = w_gate.shape[2]

    channels = conv_result.shape[0]
    channel_total = channels * tp_count
    positions = conv_result.shape[1]

    ids = jnp.stack([core, chip % 2]).astype(jnp.int32)
    w_own = local_kernel(
        functools.partial(pack_weights, chips),
        shaped((3, width, hid), bf16),
        ids,
        w_gate[0],
        w_up[0],
        w_down[0],
        specs=[SMEM, VMEM, VMEM, VMEM],
    )
    w_far = swap_chips(w_own)

    sent, slots = local_kernel(
        functools.partial(prepare, experts, capacity, share, chips),
        (shaped((experts * share, width), bf16), shaped((top, tokens), jnp.int32)),
        ids,
        route_experts.T,
        route_weights.T,
        stream_in,
        out_cot,
        specs=[SMEM, VMEM, VMEM, VMEM, VMEM],
    )
    mine = lax.all_to_all(sent.reshape(experts, share, width), "sp", 0, 0, tiled=True)
    mine = mine.reshape(rows, width)
    other = swap_cores(mine)

    far_rows = swap_chips(mine)

    own_acts, far_acts, back_mine, back_other = local_kernel(
        experts_step,
        (
            shaped((3, rows, hid), bf16),
            shaped((3, rows, hid), bf16),
            shaped((rows, half), f32),
            shaped((rows, half), bf16),
        ),
        mine,
        other,
        w_own,
        w_far,
    )
    from_core = swap_cores(back_other)
    back = (back_mine + from_core.astype(f32)).astype(bf16)
    back = back.reshape(sp_count, share, chips, cols).transpose(0, 2, 1, 3)
    back = back.reshape(sp_count * chips, share, cols)
    back, own_acts, far_acts = lax.optimization_barrier((back, own_acts, far_acts))
    returned = lax.all_to_all(back, ("sp", "chip"), 0, 0, tiled=True)

    far_acts = swap_chips(far_acts)
    far_other = swap_cores(far_rows)
    gate, up, down = local_kernel(
        functools.partial(weight_grads, chips),
        (shaped((width, hid), bf16), shaped((width, hid), bf16), shaped((hid, width), bf16)),
        ids,
        mine,
        other,
        far_rows,
        far_other,
        own_acts,
        far_acts,
        specs=[SMEM] + [VMEM] * 6,
    )
    grad_gate, grad_up, grad_down = gate[None], up[None], down[None]

    cot_cols = lax.dynamic_slice_in_dim(out_cot, tp * cols, cols, 1)
    payload = local_kernel(
        functools.partial(finish, capacity, share, chips),
        shaped((tokens + 16, cols), bf16),
        returned.reshape(experts * chips * share, cols),
        slots,
        cot_cols,
        conv_result,
    )
    got = lax.all_gather(payload, TP)

    xhat, centred, inverse, sums, grad_stream, packed = local_kernel(
        functools.partial(tail, channel_total),
        (
            shaped((channels, positions), f32),
            shaped((channels, positions), f32),
            shaped((1, positions), f32),
            shaped((tp_count, 8, positions), f32),
            shaped((tokens, width), bf16),
            shaped((sp_count, 32, 2 * channels), bf16),
        ),
        got,
        w_proj.T,
        conv_result,
        channel_norm_gain[:, None],
    )
    sums = lax.all_to_all(sums, TP, 0, 0, tiled=True)
    grad_conv = local_kernel(
        functools.partial(normalise, channel_total),
        shaped((channels, positions), f32),
        sums,
        xhat,
        centred,
        inverse,
    )

    packed = lax.all_to_all(packed, "sp", 0, 0, tiled=True)
    total = jnp.sum(packed.astype(f32), axis=0)
    grad_proj = jnp.concatenate([total[:, :channels], total[:, channels:]], axis=0)

    rim = lax.ppermute(grad_conv, "sp", [(k, k - 1) for k in range(1, sp_count)])
    grad_value, grad_gate_in = local_kernel(
        convolve,
        (shaped((channels, positions), bf16), shaped((channels, positions), bf16)),
        grad_conv,
        rim,
        conv_taps.T,
        conv_gate,
        conv_value,
    )
    return (grad_gate, grad_up, grad_down, grad_stream, grad_proj, grad_value, grad_gate_in)


def solution(mesh):
    sp_count = mesh.shape["sp"]
    devices = mesh.devices.reshape(sp_count, -1, 2)
    return jax.shard_map(
        body,
        mesh=Mesh(devices, ("sp", "chip", "core")),
        in_specs=(
            P("sp", None),
            P("sp", None),
            P("sp", None),
            P("sp", None),
            P("sp", None, TP),
            P("sp", None, TP),
            P("sp", TP, None),
            P(None, TP),
            P(TP, "sp"),
            P(TP, "sp"),
            P(None, TP),
            P(TP, "sp"),
            P(TP),
        ),
        out_specs=(
            P("sp", None, TP),
            P("sp", None, TP),
            P("sp", TP, None),
            P("sp", None),
            P("sp", TP),
            P(TP, "sp"),
            P(TP, "sp"),
        ),
        check_vma=False,
    )
```

```python
import functools

import jax
import jax.numpy as jnp
from jax import lax
from jax.experimental import pallas as pl
from jax.experimental.pallas import tpu as pltpu
from jax.sharding import Mesh
from jax.sharding import PartitionSpec as P


norm_eps = 1e-05
clamp_limit = 7.0
alpha_gate = 1.702
bf16 = jnp.bfloat16
f32 = jnp.float32
LANES = 128


TP = ("chip", "core")
VMEM = pl.BlockSpec(memory_space=pltpu.VMEM)
SMEM = pl.BlockSpec(memory_space=pltpu.SMEM)


def dot(a, b, dims):
    return lax.dot_general(a, b, (dims, ((), ())), preferred_element_type=f32)


NN = ((1,), (0,))
NT = ((1,), (1,))
TN = ((0,), (0,))


def local_kernel(body, outs, *args, specs=None, flops=10**9):
    size = sum(a.size * a.dtype.itemsize for a in args)
    return pl.pallas_call(
        body,
        out_shape=outs,
        in_specs=[VMEM] * len(args) if specs is None else specs,
        out_specs=jax.tree.map(lambda _: VMEM, outs),
        cost_estimate=pl.CostEstimate(flops=flops, bytes_accessed=size, transcendentals=0),
        compiler_params=pltpu.CompilerParams(vmem_limit_bytes=40 * 2**20),
    )(*args)


def shaped(shape, dtype):
    return jax.ShapeDtypeStruct(shape, dtype)


def swap_cores(value):
    return lax.ppermute(value, "core", [(0, 1), (1, 0)])


def swap_chips(value):
    count = lax.axis_size("chip")
    return lax.ppermute(value, "chip", [(k, k ^ 1) for k in range(count)])


def pack_weights(chips, ids, gate, up, down, out):
    half = chips * LANES
    for turn in range(2):
        which = ids[0] if turn == 0 else 1 - ids[0]
        for i in range(chips):
            at = pl.ds(pl.multiple_of((2 * i + which) * LANES, LANES), LANES)
            here = slice(turn * half + i * LANES, turn * half + (i + 1) * LANES)
            out[0, here, :] = gate[at, :]
            out[1, here, :] = up[at, :]
            out[2, here, :] = down[:, at]


def prepare(experts, capacity, share, chips, ids, routes, weights, stream, cot, out, slots):
    top, count = routes.shape
    core, part = ids[0], ids[1]
    before = (
        lax.broadcasted_iota(jnp.int32, (count, count), 0)
        < lax.broadcasted_iota(jnp.int32, (count, count), 1)
    ).astype(bf16)
    named = lax.broadcasted_iota(jnp.int32, (experts, count), 0)
    row = lax.broadcasted_iota(jnp.int32, (experts * share, count), 0)
    base = jnp.zeros((experts, 1), f32)
    picked = jnp.zeros((experts * share, count), jnp.bool_)
    weight = jnp.zeros((experts * share, count), f32)
    for k in range(top):
        route = routes[k : k + 1, :]
        hot = named == route
        ones = jnp.where(hot, 1.0, 0.0)
        ahead = dot(ones.astype(bf16), before, NN) + base
        base = base + jnp.sum(ones, axis=1, keepdims=True)
        rank = jnp.sum(jnp.where(hot, ahead, 0.0), axis=0, keepdims=True).astype(jnp.int32)
        slots[k : k + 1, :] = route * capacity + rank
        local = rank - part * share
        held = (local >= 0) & (local < share)
        mine = row == jnp.where(held, route * share + local, -1)
        picked = picked | mine
        weight = weight + jnp.where(mine, weights[k : k + 1, :], 0.0)
    choice = jnp.where(picked, 1.0, 0.0).astype(bf16)
    scale = jnp.sum(weight, axis=1, keepdims=True)
    half = chips * LANES
    for i in range(chips):
        at = pl.ds(pl.multiple_of((2 * i + core) * LANES, LANES), LANES)
        out[:, i * LANES : (i + 1) * LANES] = dot(choice, stream[:, at], NN).astype(bf16)
        got = dot(choice, cot[:, at], NN)
        out[:, half + i * LANES : half + (i + 1) * LANES] = (scale * got).astype(bf16)


def experts_step(mine, other, own, far, own_acts, far_acts, back_mine, back_other):
    half = mine.shape[1] // 2
    for w, acts in ((own, own_acts), (far, far_acts)):

        def product(n, at):
            return dot(mine[:, at : at + half], w[n, :half], NN) + dot(
                other[:, at : at + half], w[n, half:], NN
            )

        pre_gate, pre_up = product(0, 0), product(1, 0)
        grad_act = 0.0
        for i in range(half // LANES):
            here, there = i * LANES, half + i * LANES
            block = slice(there, there + LANES)
            grad_act = grad_act + dot(mine[:, block], w[2, here : here + LANES], NT)
            grad_act = grad_act + dot(other[:, block], w[2, there : there + LANES], NT)
        glu = jnp.minimum(pre_gate, clamp_limit)
        lin = jnp.clip(pre_up, -clamp_limit, clamp_limit)
        sig = jax.nn.sigmoid(alpha_gate * glu)
        slope = sig + alpha_gate * glu * sig * (1.0 - sig)
        acts[2] = (glu * sig * (lin + 1.0)).astype(bf16)
        acts[0] = jnp.where(
            pre_gate < clamp_limit, grad_act * (lin + 1.0) * slope, 0.0
        ).astype(bf16)
        acts[1] = jnp.where(
            jnp.abs(pre_up) < clamp_limit, grad_act * glu * sig, 0.0
        ).astype(bf16)

    def back(at):
        total = 0.0
        for w, acts in ((own, own_acts), (far, far_acts)):
            total = total + dot(acts[0], w[0, at : at + half], NT)
            total = total + dot(acts[1], w[1, at : at + half], NT)
        return total

    back_other[...] = back(half).astype(bf16)
    back_mine[...] = back(0)


def weight_grads(chips, ids, mine, other, far, far_other, own_acts, far_acts, gate, up, down):
    core = ids[0]
    half = chips * LANES
    for turn, (near_rows, far_rows) in enumerate(((mine, far), (other, far_other))):
        which = core if turn == 0 else 1 - core
        for i in range(chips):
            at = pl.ds(pl.multiple_of((2 * i + which) * LANES, LANES), LANES)
            here = slice(i * LANES, (i + 1) * LANES)
            there = slice(half + i * LANES, half + (i + 1) * LANES)
            near, away = near_rows[:, here], far_rows[:, here]
            for n, out in enumerate((gate, up)):
                total = dot(near, own_acts[n], TN) + dot(away, far_acts[n], TN)
                out[at, :] = total.astype(bf16)
            total = dot(own_acts[2], near_rows[:, there], TN)
            total = total + dot(far_acts[2], far_rows[:, there], TN)
            down[:, at] = total.astype(bf16)


def in_parts(x):
    high = x.astype(bf16).astype(f32)
    middle = (x - high).astype(bf16).astype(f32)
    return high, middle, x - high - middle


def finish(capacity, share, chips, ids, data, slots, cot, conv, out):
    rows, count = data.shape[0], slots.shape[1]
    row = lax.broadcasted_iota(jnp.int32, (rows, count), 0)
    expert = row // (chips * share)
    chip = (row // share) % chips
    key = expert * capacity + (chip % 2) * share + row % share
    hit = (key == slots[0:1, :]) | (key == slots[1:2, :])
    total = dot(jnp.where(hit, 1.0, 0.0).astype(bf16), data[...], TN)
    at = pl.ds(pl.multiple_of(ids[2] * LANES, LANES), LANES)
    out[0:count, :] = (cot[:, at].astype(f32) + total).astype(bf16)
    wide = conv[...].astype(f32)
    at = lax.broadcasted_iota(jnp.int32, (16, count), 0)
    block = jnp.zeros((16, count), f32)
    sums = jnp.sum(wide, axis=0, keepdims=True), jnp.sum(wide * wide, axis=0, keepdims=True)
    for n, x in enumerate(in_parts(sums[0]) + in_parts(sums[1])):
        block = jnp.where(at == n, x, block)
    out[count : count + 16, :] = block.astype(bf16)


def tail(total_channels, got, proj_t, conv, gain, xhat, centred, inverse, sums, stream, packed):
    pieces, count = got.shape[0], stream.shape[0]
    channels = proj_t.shape[0]
    lane = lax.broadcasted_iota(jnp.int32, (32, 2 * channels), 1)
    parts = jnp.zeros((16, count), f32)
    for j in range(pieces):
        parts = parts + got[j, count : count + 16, :].astype(f32)
    mean = (parts[0:1] + parts[1:2] + parts[2:3]) / total_channels
    square = (parts[3:4] + parts[4:5] + parts[5:6]) / total_channels
    scale = lax.rsqrt(square - mean * mean + norm_eps)
    removed = (conv[...].astype(f32) - mean) * scale
    normed = removed * gain[...]
    sig = jax.nn.sigmoid(normed)
    hidden = normed * sig
    hid_t = jnp.concatenate([hidden, hidden]).T.astype(bf16)
    hidden_grad = jnp.zeros((channels, count), f32)
    for j in range(pieces):
        part = got[j, :count, :]
        stream[:, j * LANES : (j + 1) * LANES] = part
        hidden_grad = hidden_grad + dot(proj_t[:, j * LANES : (j + 1) * LANES], part, NT)
        outer = dot(part, hid_t, TN)
        for u in range(2):
            first = outer[64 * u : 64 * u + 32]
            second = outer[64 * u + 32 : 64 * u + 64]
            packed[2 * j + u] = jnp.where(lane < channels, first, second).astype(bf16)
    grown = hidden_grad * sig * (1.0 + normed * (1.0 - sig)) * gain[...]
    xhat[...] = grown
    centred[...] = removed
    inverse[...] = scale
    at = lax.broadcasted_iota(jnp.int32, (8, count), 0)
    one = jnp.sum(grown, axis=0, keepdims=True)
    two = jnp.sum(grown * removed, axis=0, keepdims=True)
    block = jnp.where(at == 0, one, jnp.where(at == 1, two, 0.0))
    for j in range(pieces):
        sums[j] = block


def normalise(total_channels, sums, xhat, centred, inverse, conv):
    block = jnp.zeros(sums.shape[1:], f32)
    for j in range(sums.shape[0]):
        block = block + sums[j]
    block = block / total_channels
    conv[...] = inverse[...] * (xhat[...] - block[0:1] - centred[...] * block[1:2])


def convolve(conv, rim, taps, gate, value, grad_value, grad_gate_in):
    count = conv.shape[1]
    lane = lax.broadcasted_iota(jnp.int32, conv.shape, 1)
    near, after = conv[...], rim[...]
    total = taps[:, 0:1] * near
    for tap in range(1, taps.shape[1]):
        shifted = jnp.where(
            lane < count - tap,
            pltpu.roll(near, count - tap, 1),
            pltpu.roll(after, count - tap, 1),
        )
        total = total + taps[:, tap : tap + 1] * shifted
    sig = jax.nn.sigmoid(gate[...].astype(f32))
    grad_value[...] = (total * sig).astype(bf16)
    grad_gate_in[...] = (total * value[...].astype(f32) * sig * (1.0 - sig)).astype(bf16)


def body(
    stream_in,
    out_cot,
    route_experts,
    route_weights,
    w_gate,
    w_up,
    w_down,
    w_proj,
    conv_value,
    conv_gate,
    conv_taps,
    conv_result,
    channel_norm_gain,
):
    sp_count = lax.axis_size("sp")
    chips = lax.axis_size("chip")
    core = lax.axis_index("core")
    chip = lax.axis_index("chip")
    tp_count = 2 * chips
    experts = w_gate.shape[0] * sp_count
    tokens, width = stream_in.shape
    top = route_experts.shape[1]
    capacity = 2 * top * tokens // experts
    share = capacity // 2
    rows = sp_count * share
    half = width // 2
    cols = width // tp_count
    hid = w_gate.shape[2]

    channels = conv_result.shape[0]
    channel_total = channels * tp_count
    positions = conv_result.shape[1]

    ids = jnp.stack([core, chip % 2, 2 * chip + core]).astype(jnp.int32)
    w_own = local_kernel(
        functools.partial(pack_weights, chips),
        shaped((3, width, hid), bf16),
        ids,
        w_gate[0],
        w_up[0],
        w_down[0],
        specs=[SMEM, VMEM, VMEM, VMEM],
    )
    w_far = swap_chips(w_own)

    sent, slots = local_kernel(
        functools.partial(prepare, experts, capacity, share, chips),
        (shaped((experts * share, width), bf16), shaped((top, tokens), jnp.int32)),
        ids,
        route_experts.T,
        route_weights.T,
        stream_in,
        out_cot,
        specs=[SMEM, VMEM, VMEM, VMEM, VMEM],
    )
    mine = lax.all_to_all(sent.reshape(experts, share, width), "sp", 0, 0, tiled=True)
    mine = mine.reshape(rows, width)
    other = swap_cores(mine)

    far_rows = swap_chips(mine)

    own_acts, far_acts, back_mine, back_other = local_kernel(
        experts_step,
        (
            shaped((3, rows, hid), bf16),
            shaped((3, rows, hid), bf16),
            shaped((rows, half), f32),
            shaped((rows, half), bf16),
        ),
        mine,
        other,
        w_own,
        w_far,
    )
    from_core = swap_cores(back_other)
    back = (back_mine + from_core.astype(f32)).astype(bf16)
    back = back.reshape(sp_count, share, chips, cols).transpose(0, 2, 1, 3)
    back = back.reshape(sp_count * chips, share, cols)
    back, own_acts, far_acts = lax.optimization_barrier((back, own_acts, far_acts))
    returned = lax.all_to_all(back, ("sp", "chip"), 0, 0, tiled=True)

    far_acts = swap_chips(far_acts)
    far_other = swap_cores(far_rows)
    gate, up, down = local_kernel(
        functools.partial(weight_grads, chips),
        (shaped((width, hid), bf16), shaped((width, hid), bf16), shaped((hid, width), bf16)),
        ids,
        mine,
        other,
        far_rows,
        far_other,
        own_acts,
        far_acts,
        specs=[SMEM] + [VMEM] * 6,
    )
    grad_gate, grad_up, grad_down = gate[None], up[None], down[None]

    payload = local_kernel(
        functools.partial(finish, capacity, share, chips),
        shaped((tokens + 16, cols), bf16),
        ids,
        returned.reshape(experts * chips * share, cols),
        slots,
        out_cot,
        conv_result,
        specs=[SMEM] + [VMEM] * 4,
    )
    got = lax.all_gather(payload, TP)

    xhat, centred, inverse, sums, grad_stream, packed = local_kernel(
        functools.partial(tail, channel_total),
        (
            shaped((channels, positions), f32),
            shaped((channels, positions), f32),
            shaped((1, positions), f32),
            shaped((tp_count, 8, positions), f32),
            shaped((tokens, width), bf16),
            shaped((sp_count, 32, 2 * channels), bf16),
        ),
        got,
        w_proj.T,
        conv_result,
        channel_norm_gain[:, None],
    )
    sums = lax.all_to_all(sums, TP, 0, 0, tiled=True)
    grad_conv = local_kernel(
        functools.partial(normalise, channel_total),
        shaped((channels, positions), f32),
        sums,
        xhat,
        centred,
        inverse,
    )

    packed = lax.all_to_all(packed, "sp", 0, 0, tiled=True)
    total = jnp.sum(packed.astype(f32), axis=0)
    grad_proj = jnp.concatenate([total[:, :channels], total[:, channels:]], axis=0)

    rim = lax.ppermute(grad_conv, "sp", [(k, k - 1) for k in range(1, sp_count)])
    grad_value, grad_gate_in = local_kernel(
        convolve,
        (shaped((channels, positions), bf16), shaped((channels, positions), bf16)),
        grad_conv,
        rim,
        conv_taps.T,
        conv_gate,
        conv_value,
    )
    return (grad_gate, grad_up, grad_down, grad_stream, grad_proj, grad_value, grad_gate_in)


def solution(mesh):
    sp_count = mesh.shape["sp"]
    devices = mesh.devices.reshape(sp_count, -1, 2)
    return jax.shard_map(
        body,
        mesh=Mesh(devices, ("sp", "chip", "core")),
        in_specs=(
            P("sp", None),
            P("sp", None),
            P("sp", None),
            P("sp", None),
            P("sp", None, TP),
            P("sp", None, TP),
            P("sp", TP, None),
            P(None, TP),
            P(TP, "sp"),
            P(TP, "sp"),
            P(None, TP),
            P(TP, "sp"),
            P(TP),
        ),
        out_specs=(
            P("sp", None, TP),
            P("sp", None, TP),
            P("sp", TP, None),
            P("sp", None),
            P("sp", TP),
            P(TP, "sp"),
            P(TP, "sp"),
        ),
        check_vma=False,
    )
```

```python
import functools

import jax
import jax.numpy as jnp
from jax import lax
from jax.experimental import pallas as pl
from jax.experimental.pallas import tpu as pltpu
from jax.sharding import Mesh
from jax.sharding import PartitionSpec as P


norm_eps = 1e-05
clamp_limit = 7.0
alpha_gate = 1.702
bf16 = jnp.bfloat16
f32 = jnp.float32
LANES = 128


TP = ("chip", "core")
VMEM = pl.BlockSpec(memory_space=pltpu.VMEM)
SMEM = pl.BlockSpec(memory_space=pltpu.SMEM)
HBM = pl.BlockSpec(memory_space=pltpu.HBM)


def dot(a, b, dims):
    return lax.dot_general(a, b, (dims, ((), ())), preferred_element_type=f32)


NN = ((1,), (0,))
NT = ((1,), (1,))
TN = ((0,), (0,))


def local_kernel(body, outs, *args, specs=None, scratch=(), grant=16, flops=10**9):
    size = sum(a.size * a.dtype.itemsize for a in args)
    return pl.pallas_call(
        body,
        out_shape=outs,
        in_specs=[VMEM] * len(args) if specs is None else specs,
        out_specs=jax.tree.map(lambda _: VMEM, outs),
        cost_estimate=pl.CostEstimate(flops=flops, bytes_accessed=size, transcendentals=0),
        compiler_params=pltpu.CompilerParams(vmem_limit_bytes=grant * 2**20),
        scratch_shapes=scratch,
    )(*args)


def shaped(shape, dtype):
    return jax.ShapeDtypeStruct(shape, dtype)


def swap_cores(value):
    return lax.ppermute(value, "core", [(0, 1), (1, 0)])


def swap_chips(value):
    count = lax.axis_size("chip")
    return lax.ppermute(value, "chip", [(k, k ^ 1) for k in range(count)])


def pack_weights(chips, ids, gate, up, down, out, sems):
    half = chips * LANES
    copies = []
    for turn in range(2):
        which = ids[0] if turn == 0 else 1 - ids[0]
        for i in range(chips):
            at = pl.ds(pl.multiple_of((2 * i + which) * LANES, LANES), LANES)
            here = slice(turn * half + i * LANES, turn * half + (i + 1) * LANES)
            for n, block in enumerate((gate.at[0, at, :], up.at[0, at, :], down.at[0, :, at])):
                sem = sems.at[len(copies)]
                copies.append(pltpu.make_async_copy(block, out.at[n, here, :], sem))
                copies[-1].start()
    for copy in copies:
        copy.wait()


def prepare(experts, capacity, share, chips, ids, routes, weights, stream, cot, out, slots):
    top, count = routes.shape
    core, part = ids[0], ids[1]
    before = (
        lax.broadcasted_iota(jnp.int32, (count, count), 0)
        < lax.broadcasted_iota(jnp.int32, (count, count), 1)
    ).astype(bf16)
    named = lax.broadcasted_iota(jnp.int32, (experts, count), 0)
    row = lax.broadcasted_iota(jnp.int32, (experts * share, count), 0)
    base = jnp.zeros((experts, 1), f32)
    picked = jnp.zeros((experts * share, count), jnp.bool_)
    weight = jnp.zeros((experts * share, count), f32)
    for k in range(top):
        route = routes[k : k + 1, :]
        hot = named == route
        ones = jnp.where(hot, 1.0, 0.0)
        ahead = dot(ones.astype(bf16), before, NN) + base
        base = base + jnp.sum(ones, axis=1, keepdims=True)
        rank = jnp.sum(jnp.where(hot, ahead, 0.0), axis=0, keepdims=True).astype(jnp.int32)
        slots[k : k + 1, :] = route * capacity + rank
        local = rank - part * share
        held = (local >= 0) & (local < share)
        mine = row == jnp.where(held, route * share + local, -1)
        picked = picked | mine
        weight = weight + jnp.where(mine, weights[k : k + 1, :], 0.0)
    choice = jnp.where(picked, 1.0, 0.0).astype(bf16)
    scale = jnp.sum(weight, axis=1, keepdims=True)
    half = chips * LANES
    for i in range(chips):
        at = pl.ds(pl.multiple_of((2 * i + core) * LANES, LANES), LANES)
        out[:, i * LANES : (i + 1) * LANES] = dot(choice, stream[:, at], NN).astype(bf16)
        got = dot(choice, cot[:, at], NN)
        out[:, half + i * LANES : half + (i + 1) * LANES] = (scale * got).astype(bf16)


def experts_step(mine, other, own, far, own_acts, far_acts, back_mine, back_other):
    half = mine.shape[1] // 2
    for w, acts in ((own, own_acts), (far, far_acts)):

        def product(n, at):
            return dot(mine[:, at : at + half], w[n, :half], NN) + dot(
                other[:, at : at + half], w[n, half:], NN
            )

        pre_gate, pre_up = product(0, 0), product(1, 0)
        grad_act = 0.0
        for i in range(half // LANES):
            here, there = i * LANES, half + i * LANES
            block = slice(there, there + LANES)
            grad_act = grad_act + dot(mine[:, block], w[2, here : here + LANES], NT)
            grad_act = grad_act + dot(other[:, block], w[2, there : there + LANES], NT)
        glu = jnp.minimum(pre_gate, clamp_limit)
        lin = jnp.clip(pre_up, -clamp_limit, clamp_limit)
        sig = jax.nn.sigmoid(alpha_gate * glu)
        slope = sig + alpha_gate * glu * sig * (1.0 - sig)
        acts[2] = (glu * sig * (lin + 1.0)).astype(bf16)
        acts[0] = jnp.where(
            pre_gate < clamp_limit, grad_act * (lin + 1.0) * slope, 0.0
        ).astype(bf16)
        acts[1] = jnp.where(
            jnp.abs(pre_up) < clamp_limit, grad_act * glu * sig, 0.0
        ).astype(bf16)

    def back(at):
        total = 0.0
        for w, acts in ((own, own_acts), (far, far_acts)):
            total = total + dot(acts[0], w[0, at : at + half], NT)
            total = total + dot(acts[1], w[1, at : at + half], NT)
        return total

    back_other[...] = back(half).astype(bf16)
    back_mine[...] = back(0)


def weight_grads(chips, ids, mine, other, far, far_other, own_acts, far_acts, gate, up, down):
    core = ids[0]
    half = chips * LANES
    for turn, (near_rows, far_rows) in enumerate(((mine, far), (other, far_other))):
        which = core if turn == 0 else 1 - core
        for i in range(chips):
            at = pl.ds(pl.multiple_of((2 * i + which) * LANES, LANES), LANES)
            here = slice(i * LANES, (i + 1) * LANES)
            there = slice(half + i * LANES, half + (i + 1) * LANES)
            near, away = near_rows[:, here], far_rows[:, here]
            for n, out in enumerate((gate, up)):
                total = dot(near, own_acts[n], TN) + dot(away, far_acts[n], TN)
                out[at, :] = total.astype(bf16)
            total = dot(own_acts[2], near_rows[:, there], TN)
            total = total + dot(far_acts[2], far_rows[:, there], TN)
            down[:, at] = total.astype(bf16)


def in_parts(x):
    high = x.astype(bf16).astype(f32)
    middle = (x - high).astype(bf16).astype(f32)
    return high, middle, x - high - middle


def finish(capacity, share, chips, ids, data, slots, cot, conv, out, cot_here, conv_here, sems):
    rows, count = data.shape[0], slots.shape[1]
    columns = pl.ds(pl.multiple_of(ids[2] * LANES, LANES), LANES)
    cot_copy = pltpu.make_async_copy(cot.at[:, columns], cot_here, sems.at[0])
    conv_copy = pltpu.make_async_copy(conv, conv_here, sems.at[1])
    cot_copy.start()
    conv_copy.start()
    row = lax.broadcasted_iota(jnp.int32, (rows, count), 0)
    expert = row // (chips * share)
    chip = (row // share) % chips
    key = expert * capacity + (chip % 2) * share + row % share
    hit = (key == slots[0:1, :]) | (key == slots[1:2, :])
    total = dot(jnp.where(hit, 1.0, 0.0).astype(bf16), data[...], TN)
    cot_copy.wait()
    out[0:count, :] = (cot_here[...].astype(f32) + total).astype(bf16)
    conv_copy.wait()
    wide = conv_here[...].astype(f32)
    at = lax.broadcasted_iota(jnp.int32, (16, count), 0)
    block = jnp.zeros((16, count), f32)
    sums = jnp.sum(wide, axis=0, keepdims=True), jnp.sum(wide * wide, axis=0, keepdims=True)
    for n, x in enumerate(in_parts(sums[0]) + in_parts(sums[1])):
        block = jnp.where(at == n, x, block)
    out[count : count + 16, :] = block.astype(bf16)


def tail(total_channels, got, proj_t, conv, gain, kept, sums, stream, packed):
    pieces, count = got.shape[0], stream.shape[0]
    channels = proj_t.shape[0]
    lane = lax.broadcasted_iota(jnp.int32, (32, 2 * channels), 1)
    parts = jnp.zeros((16, count), f32)
    for j in range(pieces):
        parts = parts + got[j, count : count + 16, :].astype(f32)
    mean = (parts[0:1] + parts[1:2] + parts[2:3]) / total_channels
    square = (parts[3:4] + parts[4:5] + parts[5:6]) / total_channels
    scale = lax.rsqrt(square - mean * mean + norm_eps)
    removed = (conv[...].astype(f32) - mean) * scale
    normed = removed * gain[...]
    sig = jax.nn.sigmoid(normed)
    hidden = normed * sig
    hid_t = jnp.concatenate([hidden, hidden]).T.astype(bf16)
    hidden_grad = jnp.zeros((channels, count), f32)
    for j in range(pieces):
        part = got[j, :count, :]
        stream[:, j * LANES : (j + 1) * LANES] = part
        hidden_grad = hidden_grad + dot(proj_t[:, j * LANES : (j + 1) * LANES], part, NT)
        outer = dot(part, hid_t, TN)
        for u in range(2):
            first = outer[64 * u : 64 * u + 32]
            second = outer[64 * u + 32 : 64 * u + 64]
            packed[2 * j + u] = jnp.where(lane < channels, first, second).astype(bf16)
    grown = hidden_grad * sig * (1.0 + normed * (1.0 - sig)) * gain[...]
    kept[0:channels] = grown
    kept[channels : 2 * channels] = removed
    kept[2 * channels :] = jnp.broadcast_to(scale, (8, count))
    at = lax.broadcasted_iota(jnp.int32, (8, count), 0)
    one = jnp.sum(grown, axis=0, keepdims=True)
    two = jnp.sum(grown * removed, axis=0, keepdims=True)
    block = jnp.where(at == 0, one, jnp.where(at == 1, two, 0.0))
    for j in range(pieces):
        sums[j] = block


def normalise(total_channels, sums, kept, conv):
    channels = conv.shape[0]
    block = jnp.zeros(sums.shape[1:], f32)
    for j in range(sums.shape[0]):
        block = block + sums[j]
    block = block / total_channels
    xhat, centred = kept[0:channels], kept[channels : 2 * channels]
    inverse = kept[2 * channels : 2 * channels + 1]
    conv[...] = inverse * (xhat - block[0:1] - centred * block[1:2])


def convolve(conv, rim, taps, gate, value, grad_value, grad_gate_in):
    count = conv.shape[1]
    lane = lax.broadcasted_iota(jnp.int32, conv.shape, 1)
    near, after = conv[...], rim[...]
    total = taps[:, 0:1] * near
    for tap in range(1, taps.shape[1]):
        shifted = jnp.where(
            lane < count - tap,
            pltpu.roll(near, count - tap, 1),
            pltpu.roll(after, count - tap, 1),
        )
        total = total + taps[:, tap : tap + 1] * shifted
    sig = jax.nn.sigmoid(gate[...].astype(f32))
    grad_value[...] = (total * sig).astype(bf16)
    grad_gate_in[...] = (total * value[...].astype(f32) * sig * (1.0 - sig)).astype(bf16)


def body(
    stream_in,
    out_cot,
    route_experts,
    route_weights,
    w_gate,
    w_up,
    w_down,
    w_proj,
    conv_value,
    conv_gate,
    conv_taps,
    conv_result,
    channel_norm_gain,
):
    sp_count = lax.axis_size("sp")
    chips = lax.axis_size("chip")
    core = lax.axis_index("core")
    chip = lax.axis_index("chip")
    tp_count = 2 * chips
    experts = w_gate.shape[0] * sp_count
    tokens, width = stream_in.shape
    top = route_experts.shape[1]
    capacity = 2 * top * tokens // experts
    share = capacity // 2
    rows = sp_count * share
    half = width // 2
    cols = width // tp_count
    hid = w_gate.shape[2]

    channels = conv_result.shape[0]
    channel_total = channels * tp_count
    positions = conv_result.shape[1]

    ids = jnp.stack([core, chip % 2, 2 * chip + core]).astype(jnp.int32)
    w_own = local_kernel(
        functools.partial(pack_weights, chips),
        shaped((3, width, hid), bf16),
        ids,
        w_gate,
        w_up,
        w_down,
        specs=[SMEM] + [HBM] * 3,
        scratch=[pltpu.SemaphoreType.DMA((3 * tp_count,))],
        grant=60,
    )
    w_far = swap_chips(w_own)

    sent, slots = local_kernel(
        functools.partial(prepare, experts, capacity, share, chips),
        (shaped((experts * share, width), bf16), shaped((top, tokens), jnp.int32)),
        ids,
        route_experts.T,
        route_weights.T,
        stream_in,
        out_cot,
        specs=[SMEM, VMEM, VMEM, VMEM, VMEM],
    )
    mine = lax.all_to_all(sent.reshape(experts, share, width), "sp", 0, 0, tiled=True)
    mine = mine.reshape(rows, width)
    other = swap_cores(mine)

    far_rows = swap_chips(mine)

    own_acts, far_acts, back_mine, back_other = local_kernel(
        experts_step,
        (
            shaped((3, rows, hid), bf16),
            shaped((3, rows, hid), bf16),
            shaped((rows, half), f32),
            shaped((rows, half), bf16),
        ),
        mine,
        other,
        w_own,
        w_far,
    )
    from_core = swap_cores(back_other)
    back = (back_mine + from_core.astype(f32)).astype(bf16)
    back = back.reshape(sp_count, share, chips, cols).transpose(0, 2, 1, 3)
    back = back.reshape(sp_count * chips, share, cols)
    back, own_acts, far_acts = lax.optimization_barrier((back, own_acts, far_acts))
    returned = lax.all_to_all(back, ("sp", "chip"), 0, 0, tiled=True)

    far_acts = swap_chips(far_acts)
    far_other = swap_cores(far_rows)
    gate, up, down = local_kernel(
        functools.partial(weight_grads, chips),
        (shaped((width, hid), bf16), shaped((width, hid), bf16), shaped((hid, width), bf16)),
        ids,
        mine,
        other,
        far_rows,
        far_other,
        own_acts,
        far_acts,
        specs=[SMEM] + [VMEM] * 6,
    )
    grad_gate, grad_up, grad_down = gate[None], up[None], down[None]

    payload = local_kernel(
        functools.partial(finish, capacity, share, chips),
        shaped((tokens + 16, cols), bf16),
        ids,
        returned.reshape(experts * chips * share, cols),
        slots,
        out_cot,
        conv_result,
        specs=[SMEM, VMEM, VMEM, HBM, HBM],
        scratch=[
            pltpu.VMEM((tokens, cols), bf16),
            pltpu.VMEM((channels, positions), bf16),
            pltpu.SemaphoreType.DMA((2,)),
        ],
        grant=60,
    )
    got = lax.all_gather(payload, TP)

    kept, sums, grad_stream, packed = local_kernel(
        functools.partial(tail, channel_total),
        (
            shaped((2 * channels + 8, positions), f32),
            shaped((tp_count, 8, positions), f32),
            shaped((tokens, width), bf16),
            shaped((sp_count, 32, 2 * channels), bf16),
        ),
        got,
        w_proj.T,
        conv_result,
        channel_norm_gain[:, None],
    )
    sums = lax.all_to_all(sums, TP, 0, 0, tiled=True)
    grad_conv = local_kernel(
        functools.partial(normalise, channel_total),
        shaped((channels, positions), f32),
        sums,
        kept,
    )

    packed = lax.all_to_all(packed, "sp", 0, 0, tiled=True)
    total = jnp.sum(packed.astype(f32), axis=0)
    grad_proj = jnp.concatenate([total[:, :channels], total[:, channels:]], axis=0)

    rim = lax.ppermute(grad_conv, "sp", [(k, k - 1) for k in range(1, sp_count)])
    grad_value, grad_gate_in = local_kernel(
        convolve,
        (shaped((channels, positions), bf16), shaped((channels, positions), bf16)),
        grad_conv,
        rim,
        conv_taps.T,
        conv_gate,
        conv_value,
    )
    return (grad_gate, grad_up, grad_down, grad_stream, grad_proj, grad_value, grad_gate_in)


def solution(mesh):
    sp_count = mesh.shape["sp"]
    devices = mesh.devices.reshape(sp_count, -1, 2)
    return jax.shard_map(
        body,
        mesh=Mesh(devices, ("sp", "chip", "core")),
        in_specs=(
            P("sp", None),
            P("sp", None),
            P("sp", None),
            P("sp", None),
            P("sp", None, TP),
            P("sp", None, TP),
            P("sp", TP, None),
            P(None, TP),
            P(TP, "sp"),
            P(TP, "sp"),
            P(None, TP),
            P(TP, "sp"),
            P(TP),
        ),
        out_specs=(
            P("sp", None, TP),
            P("sp", None, TP),
            P("sp", TP, None),
            P("sp", None),
            P("sp", TP),
            P(TP, "sp"),
            P(TP, "sp"),
        ),
        check_vma=False,
    )
```

```python
import functools

import jax
import jax.numpy as jnp
from jax import lax
from jax.experimental import pallas as pl
from jax.experimental.pallas import tpu as pltpu
from jax.sharding import Mesh
from jax.sharding import PartitionSpec as P


norm_eps = 1e-05
clamp_limit = 7.0
alpha_gate = 1.702
bf16 = jnp.bfloat16
f32 = jnp.float32
LANES = 128


TP = ("chip", "core")
VMEM = pl.BlockSpec(memory_space=pltpu.VMEM)
SMEM = pl.BlockSpec(memory_space=pltpu.SMEM)
HBM = pl.BlockSpec(memory_space=pltpu.HBM)


def dot(a, b, dims):
    return lax.dot_general(a, b, (dims, ((), ())), preferred_element_type=f32)


NN = ((1,), (0,))
NT = ((1,), (1,))
TN = ((0,), (0,))


def local_kernel(body, outs, *args, specs=None, scratch=(), grant=16, flops=10**9):
    size = sum(a.size * a.dtype.itemsize for a in args)
    return pl.pallas_call(
        body,
        out_shape=outs,
        in_specs=[VMEM] * len(args) if specs is None else specs,
        out_specs=jax.tree.map(lambda _: VMEM, outs),
        cost_estimate=pl.CostEstimate(flops=flops, bytes_accessed=size, transcendentals=0),
        compiler_params=pltpu.CompilerParams(vmem_limit_bytes=grant * 2**20),
        scratch_shapes=scratch,
    )(*args)


def shaped(shape, dtype):
    return jax.ShapeDtypeStruct(shape, dtype)


def swap_cores(value):
    return lax.ppermute(value, "core", [(0, 1), (1, 0)])


def swap_chips(value):
    count = lax.axis_size("chip")
    return lax.ppermute(value, "chip", [(k, k ^ 1) for k in range(count)])


def prepare(experts, capacity, share, chips, ids, routes, weights, stream, cot, out, slots):
    top, count = routes.shape
    core, part = ids[0], ids[1]
    before = (
        lax.broadcasted_iota(jnp.int32, (count, count), 0)
        < lax.broadcasted_iota(jnp.int32, (count, count), 1)
    ).astype(bf16)
    named = lax.broadcasted_iota(jnp.int32, (experts, count), 0)
    row = lax.broadcasted_iota(jnp.int32, (experts * share, count), 0)
    base = jnp.zeros((experts, 1), f32)
    picked = jnp.zeros((experts * share, count), jnp.bool_)
    weight = jnp.zeros((experts * share, count), f32)
    for k in range(top):
        route = routes[k : k + 1, :]
        hot = named == route
        ones = jnp.where(hot, 1.0, 0.0)
        ahead = dot(ones.astype(bf16), before, NN) + base
        base = base + jnp.sum(ones, axis=1, keepdims=True)
        rank = jnp.sum(jnp.where(hot, ahead, 0.0), axis=0, keepdims=True).astype(jnp.int32)
        slots[k : k + 1, :] = route * capacity + rank
        local = rank - part * share
        held = (local >= 0) & (local < share)
        mine = row == jnp.where(held, route * share + local, -1)
        picked = picked | mine
        weight = weight + jnp.where(mine, weights[k : k + 1, :], 0.0)
    choice = jnp.where(picked, 1.0, 0.0).astype(bf16)
    scale = jnp.sum(weight, axis=1, keepdims=True)
    half = chips * LANES
    for i in range(chips):
        at = pl.ds(pl.multiple_of((2 * i + core) * LANES, LANES), LANES)
        out[:, i * LANES : (i + 1) * LANES] = dot(choice, stream[:, at], NN).astype(bf16)
        got = dot(choice, cot[:, at], NN)
        out[:, half + i * LANES : half + (i + 1) * LANES] = (scale * got).astype(bf16)


def experts_step(ids, mine, other, *refs):
    weights, (own_acts, far_acts, back_mine, back_other) = refs[:6], refs[6:]
    half = mine.shape[1] // 2
    core = ids[0]

    def block(i, which):
        return pl.ds(pl.multiple_of((2 * i + which) * LANES, LANES), LANES)

    for (gate, up, down), acts in ((weights[:3], own_acts), (weights[3:], far_acts)):
        pre_gate = pre_up = grad_act = 0.0
        for rows, which in ((mine, core), (other, 1 - core)):
            for i in range(half // LANES):
                at = block(i, which)
                row = rows[:, i * LANES : (i + 1) * LANES]
                pre_gate = pre_gate + dot(row, gate[0, at, :], NN)
                pre_up = pre_up + dot(row, up[0, at, :], NN)
                cot = rows[:, half + i * LANES : half + (i + 1) * LANES]
                grad_act = grad_act + dot(cot, down[0, :, at], NT)
        glu = jnp.minimum(pre_gate, clamp_limit)
        lin = jnp.clip(pre_up, -clamp_limit, clamp_limit)
        sig = jax.nn.sigmoid(alpha_gate * glu)
        slope = sig + alpha_gate * glu * sig * (1.0 - sig)
        acts[2] = (glu * sig * (lin + 1.0)).astype(bf16)
        acts[0] = jnp.where(
            pre_gate < clamp_limit, grad_act * (lin + 1.0) * slope, 0.0
        ).astype(bf16)
        acts[1] = jnp.where(
            jnp.abs(pre_up) < clamp_limit, grad_act * glu * sig, 0.0
        ).astype(bf16)

    for out, which in ((back_other, 1 - core), (back_mine, core)):
        for i in range(half // LANES):
            at = block(i, which)
            total = 0.0
            for (gate, up, _), acts in ((weights[:3], own_acts), (weights[3:], far_acts)):
                total = total + dot(acts[0], gate[0, at, :], NT)
                total = total + dot(acts[1], up[0, at, :], NT)
            out[:, i * LANES : (i + 1) * LANES] = total.astype(out.dtype)


def weight_grads(chips, ids, mine, other, far, far_other, own_acts, far_acts, gate, up, down):
    core = ids[0]
    half = chips * LANES
    for turn, (near_rows, far_rows) in enumerate(((mine, far), (other, far_other))):
        which = core if turn == 0 else 1 - core
        for i in range(chips):
            at = pl.ds(pl.multiple_of((2 * i + which) * LANES, LANES), LANES)
            here = slice(i * LANES, (i + 1) * LANES)
            there = slice(half + i * LANES, half + (i + 1) * LANES)
            near, away = near_rows[:, here], far_rows[:, here]
            for n, out in enumerate((gate, up)):
                total = dot(near, own_acts[n], TN) + dot(away, far_acts[n], TN)
                out[at, :] = total.astype(bf16)
            total = dot(own_acts[2], near_rows[:, there], TN)
            total = total + dot(far_acts[2], far_rows[:, there], TN)
            down[:, at] = total.astype(bf16)


def in_parts(x):
    high = x.astype(bf16).astype(f32)
    middle = (x - high).astype(bf16).astype(f32)
    return high, middle, x - high - middle


def finish(capacity, share, chips, ids, data, slots, cot, conv, out, cot_here, conv_here, sems):
    rows, count = data.shape[0], slots.shape[1]
    columns = pl.ds(pl.multiple_of(ids[2] * LANES, LANES), LANES)
    cot_copy = pltpu.make_async_copy(cot.at[:, columns], cot_here, sems.at[0])
    conv_copy = pltpu.make_async_copy(conv, conv_here, sems.at[1])
    cot_copy.start()
    conv_copy.start()
    row = lax.broadcasted_iota(jnp.int32, (rows, count), 0)
    expert = row // (chips * share)
    chip = (row // share) % chips
    key = expert * capacity + (chip % 2) * share + row % share
    hit = (key == slots[0:1, :]) | (key == slots[1:2, :])
    total = dot(jnp.where(hit, 1.0, 0.0).astype(bf16), data[...], TN)
    cot_copy.wait()
    out[0:count, :] = (cot_here[...].astype(f32) + total).astype(bf16)
    conv_copy.wait()
    wide = conv_here[...].astype(f32)
    at = lax.broadcasted_iota(jnp.int32, (16, count), 0)
    block = jnp.zeros((16, count), f32)
    sums = jnp.sum(wide, axis=0, keepdims=True), jnp.sum(wide * wide, axis=0, keepdims=True)
    for n, x in enumerate(in_parts(sums[0]) + in_parts(sums[1])):
        block = jnp.where(at == n, x, block)
    out[count : count + 16, :] = block.astype(bf16)


def tail(total_channels, got, proj_t, conv, gain, kept, sums, stream, packed):
    pieces, count = got.shape[0], stream.shape[0]
    channels = proj_t.shape[0]
    lane = lax.broadcasted_iota(jnp.int32, (32, 2 * channels), 1)
    parts = jnp.zeros((16, count), f32)
    for j in range(pieces):
        parts = parts + got[j, count : count + 16, :].astype(f32)
    mean = (parts[0:1] + parts[1:2] + parts[2:3]) / total_channels
    square = (parts[3:4] + parts[4:5] + parts[5:6]) / total_channels
    scale = lax.rsqrt(square - mean * mean + norm_eps)
    removed = (conv[...].astype(f32) - mean) * scale
    normed = removed * gain[...]
    sig = jax.nn.sigmoid(normed)
    hidden = normed * sig
    hid_t = jnp.concatenate([hidden, hidden]).T.astype(bf16)
    hidden_grad = jnp.zeros((channels, count), f32)
    for j in range(pieces):
        part = got[j, :count, :]
        stream[:, j * LANES : (j + 1) * LANES] = part
        hidden_grad = hidden_grad + dot(proj_t[:, j * LANES : (j + 1) * LANES], part, NT)
        outer = dot(part, hid_t, TN)
        for u in range(2):
            first = outer[64 * u : 64 * u + 32]
            second = outer[64 * u + 32 : 64 * u + 64]
            packed[2 * j + u] = jnp.where(lane < channels, first, second).astype(bf16)
    grown = hidden_grad * sig * (1.0 + normed * (1.0 - sig)) * gain[...]
    kept[0:channels] = grown
    kept[channels : 2 * channels] = removed
    kept[2 * channels :] = jnp.broadcast_to(scale, (8, count))
    at = lax.broadcasted_iota(jnp.int32, (8, count), 0)
    one = jnp.sum(grown, axis=0, keepdims=True)
    two = jnp.sum(grown * removed, axis=0, keepdims=True)
    block = jnp.where(at == 0, one, jnp.where(at == 1, two, 0.0))
    for j in range(pieces):
        sums[j] = block


def normalise(total_channels, sums, kept, conv):
    channels = conv.shape[0]
    block = jnp.zeros(sums.shape[1:], f32)
    for j in range(sums.shape[0]):
        block = block + sums[j]
    block = block / total_channels
    xhat, centred = kept[0:channels], kept[channels : 2 * channels]
    inverse = kept[2 * channels : 2 * channels + 1]
    conv[...] = inverse * (xhat - block[0:1] - centred * block[1:2])


def convolve(conv, rim, taps, gate, value, grad_value, grad_gate_in):
    count = conv.shape[1]
    lane = lax.broadcasted_iota(jnp.int32, conv.shape, 1)
    near, after = conv[...], rim[...]
    total = taps[:, 0:1] * near
    for tap in range(1, taps.shape[1]):
        shifted = jnp.where(
            lane < count - tap,
            pltpu.roll(near, count - tap, 1),
            pltpu.roll(after, count - tap, 1),
        )
        total = total + taps[:, tap : tap + 1] * shifted
    sig = jax.nn.sigmoid(gate[...].astype(f32))
    grad_value[...] = (total * sig).astype(bf16)
    grad_gate_in[...] = (total * value[...].astype(f32) * sig * (1.0 - sig)).astype(bf16)


def body(
    stream_in,
    out_cot,
    route_experts,
    route_weights,
    w_gate,
    w_up,
    w_down,
    w_proj,
    conv_value,
    conv_gate,
    conv_taps,
    conv_result,
    channel_norm_gain,
):
    sp_count = lax.axis_size("sp")
    chips = lax.axis_size("chip")
    core = lax.axis_index("core")
    chip = lax.axis_index("chip")
    tp_count = 2 * chips
    experts = w_gate.shape[0] * sp_count
    tokens, width = stream_in.shape
    top = route_experts.shape[1]
    capacity = 2 * top * tokens // experts
    share = capacity // 2
    rows = sp_count * share
    half = width // 2
    cols = width // tp_count
    hid = w_gate.shape[2]

    channels = conv_result.shape[0]
    channel_total = channels * tp_count
    positions = conv_result.shape[1]

    ids = jnp.stack([core, chip % 2, 2 * chip + core]).astype(jnp.int32)
    gate_far = swap_chips(w_gate)
    up_far = swap_chips(w_up)
    down_far = swap_chips(w_down)

    gain = channel_norm_gain[:, None]

    sent, slots = local_kernel(
        functools.partial(prepare, experts, capacity, share, chips),
        (shaped((experts * share, width), bf16), shaped((top, tokens), jnp.int32)),
        ids,
        route_experts.T,
        route_weights.T,
        stream_in,
        out_cot,
        specs=[SMEM, VMEM, VMEM, VMEM, VMEM],
    )
    mine = lax.all_to_all(sent.reshape(experts, share, width), "sp", 0, 0, tiled=True)
    mine = mine.reshape(rows, width)
    other = swap_cores(mine)

    far_rows = swap_chips(mine)

    own_acts, far_acts, back_mine, back_other = local_kernel(
        experts_step,
        (
            shaped((3, rows, hid), bf16),
            shaped((3, rows, hid), bf16),
            shaped((rows, half), f32),
            shaped((rows, half), bf16),
        ),
        ids,
        mine,
        other,
        w_gate,
        w_up,
        w_down,
        gate_far,
        up_far,
        down_far,
        specs=[SMEM] + [VMEM] * 8,
    )
    from_core = swap_cores(back_other)
    back = (back_mine + from_core.astype(f32)).astype(bf16)
    back = back.reshape(sp_count, share, chips, cols).transpose(0, 2, 1, 3)
    back = back.reshape(sp_count * chips, share, cols)
    back, own_acts, far_acts = lax.optimization_barrier((back, own_acts, far_acts))
    returned = lax.all_to_all(back, ("sp", "chip"), 0, 0, tiled=True)

    far_acts = swap_chips(far_acts)
    far_other = swap_cores(far_rows)
    gate, up, down = local_kernel(
        functools.partial(weight_grads, chips),
        (shaped((width, hid), bf16), shaped((width, hid), bf16), shaped((hid, width), bf16)),
        ids,
        mine,
        other,
        far_rows,
        far_other,
        own_acts,
        far_acts,
        specs=[SMEM] + [VMEM] * 6,
    )
    grad_gate, grad_up, grad_down = gate[None], up[None], down[None]

    payload = local_kernel(
        functools.partial(finish, capacity, share, chips),
        shaped((tokens + 16, cols), bf16),
        ids,
        returned.reshape(experts * chips * share, cols),
        slots,
        out_cot,
        conv_result,
        specs=[SMEM, VMEM, VMEM, HBM, HBM],
        scratch=[
            pltpu.VMEM((tokens, cols), bf16),
            pltpu.VMEM((channels, positions), bf16),
            pltpu.SemaphoreType.DMA((2,)),
        ],
        grant=60,
    )
    got = lax.all_gather(payload, TP)

    kept, sums, grad_stream, packed = local_kernel(
        functools.partial(tail, channel_total),
        (
            shaped((2 * channels + 8, positions), f32),
            shaped((tp_count, 8, positions), f32),
            shaped((tokens, width), bf16),
            shaped((sp_count, 32, 2 * channels), bf16),
        ),
        got,
        w_proj.T,
        conv_result,
        gain,
    )
    sums = lax.all_to_all(sums, TP, 0, 0, tiled=True)
    grad_conv = local_kernel(
        functools.partial(normalise, channel_total),
        shaped((channels, positions), f32),
        sums,
        kept,
    )

    packed = lax.all_to_all(packed, "sp", 0, 0, tiled=True)
    total = jnp.sum(packed.astype(f32), axis=0)
    grad_proj = jnp.concatenate([total[:, :channels], total[:, channels:]], axis=0)

    rim = lax.ppermute(grad_conv, "sp", [(k, k - 1) for k in range(1, sp_count)])
    grad_value, grad_gate_in = local_kernel(
        convolve,
        (shaped((channels, positions), bf16), shaped((channels, positions), bf16)),
        grad_conv,
        rim,
        conv_taps.T,
        conv_gate,
        conv_value,
    )
    return (grad_gate, grad_up, grad_down, grad_stream, grad_proj, grad_value, grad_gate_in)


def solution(mesh):
    sp_count = mesh.shape["sp"]
    devices = mesh.devices.reshape(sp_count, -1, 2)
    return jax.shard_map(
        body,
        mesh=Mesh(devices, ("sp", "chip", "core")),
        in_specs=(
            P("sp", None),
            P("sp", None),
            P("sp", None),
            P("sp", None),
            P("sp", None, TP),
            P("sp", None, TP),
            P("sp", TP, None),
            P(None, TP),
            P(TP, "sp"),
            P(TP, "sp"),
            P(None, TP),
            P(TP, "sp"),
            P(TP),
        ),
        out_specs=(
            P("sp", None, TP),
            P("sp", None, TP),
            P("sp", TP, None),
            P("sp", None),
            P("sp", TP),
            P(TP, "sp"),
            P(TP, "sp"),
        ),
        check_vma=False,
    )
```
